128 devices in a mesh: ep: 128 (over z, y, x, core).
Axes of the slice: x: 4, y: 4, z: 4, core: 2. Of those that a mesh axis runs over, the one named last changes fastest.
Arguments:
- hidden: bfloat16 [1024, 2048], P('ep'), may hold values from -6 to 6
- lengths: int32 [1024], P('ep'), may hold values from 1 to 1024
- key_cache: bfloat16 [1024, 1024, 128], P('ep'), may hold values from -6 to 6
- value_cache: bfloat16 [1024, 1024, 128], P('ep'), may hold values from -6 to 6
- norm_gain: bfloat16 [2048], replicated, may hold values from 0.099609375 to 1.8984375
- w_query: bfloat16 [2048, 1024], replicated, may hold values from -0.125 to 0.125
- w_key: bfloat16 [2048, 128], replicated, may hold values from -0.125 to 0.125
- w_value: bfloat16 [2048, 128], replicated, may hold values from -0.125 to 0.125
- head_bias: float32 [16], replicated, may hold values from -7 to -2
- w_out: bfloat16 [1024, 2048], replicated, may hold values from -0.1875 to 0.1875
- ffn_gain: bfloat16 [2048], replicated, may hold values from 0.099609375 to 1.8984375
- routing: int32 [1024, 2], P('ep'), may hold values from 0 to 7, all different within a row; in each aligned block of 8 rows (0 to 7, 8 to 15, ...) at most 4 rows name the same one
- route_w: bfloat16 [1024, 2], P('ep'), may hold values from 0.19921875 to 1
- w_gate: bfloat16 [128, 2048, 352], P('ep'), may hold values from -0.125 to 0.125
- w_up: bfloat16 [128, 2048, 352], P('ep'), may hold values from -0.125 to 0.125
- w_down: bfloat16 [128, 352, 2048], P('ep'), may hold values from -0.078125 to 0.078125
Outputs:
- mixed: bfloat16 [1024, 2048], P('ep')
- new_key: bfloat16 [1024, 128], P('ep')
- new_value: bfloat16 [1024, 128], P('ep')
The draws below stay inside these ranges and needn't reach their ends.
Inputs may be any that keep to these rules, and one draw needn't show every extreme that they name: `lengths`: positions at and beyond a sequence's length are unused. `routing`: the 2 experts of a token differ; among the rows of one device at most 4 tokens name the same expert.
All inputs are finite; a program needn't handle non-finite values.
Results may differ from the reference program's by a relative error of at most 0.013.
Values may be sent and summed in bfloat16 or wider, within the bound.
A program may use at most 128 MiB of HBM per device.

```python
import math
import jax
import jax.numpy as jnp
import numpy as np
from jax import lax

D = 2048
HEADS = 16
HD = 64
KVH = 2
EXPERTS = 8
FF = 5632
TOP = 2
SEQ_DEV = 8
CACHE = 1024
CAP = 4
SLICES = 16
FF_DEV = 352
SEQS = 1024


def plant(values, rng, least, top_value):
    index_at = [jax.random.randint(jax.random.fold_in(rng, axis), (), 0, length) for axis, length in enumerate(values.shape)]
    main_axis = values.shape.index(max(values.shape))
    neighbour = index_at[:main_axis] + [(index_at[main_axis] + 1) % values.shape[main_axis]] + index_at[main_axis + 1:]
    return values.at[tuple(index_at)].set(least).at[tuple(neighbour)].set(top_value)


def block_levels(rng, dims, pieces, low, high):
    level, own = 1.0, jax.random.fold_in(rng, 6)
    for dim, blocks in pieces:
        heights = jnp.exp(jax.random.uniform(jax.random.fold_in(own, dim), (blocks,), jnp.float32, low / len(pieces), high / len(pieces)))
        level = level * jnp.repeat(heights, dims[dim] // blocks).reshape([-1 if axis == dim else 1 for axis in range(len(dims))])
    return level


def deal_out(own_key, own, number, rows, count, top, reach, slope):
    order = jax.random.permutation(own_key, count)
    heavy_load, usual = load_shares(count, rows * top, reach, slope, True), load_shares(count, rows * top, reach, slope, False)
    places = jnp.arange(count)

    def named(sizes, rotation):
        used = int((sizes > 0).sum())
        fixed = max(1, used // 4)
        moved = fixed + (places - fixed + rotation * (used - fixed)) % max(1, count - fixed)
        return jnp.zeros((count,), jnp.int32).at[order[jnp.where(places < fixed, places, moved)]].set(jnp.asarray(sizes, jnp.int32))

    sizes = jnp.where(number % 4 == 0, named(heavy_load, number // 4), named(usual, number - number // 4 - 1))
    mixed = jax.random.permutation(jax.random.fold_in(own, 3), count)
    giver, taker = mixed[0:count // 2 * 2:2], mixed[1:count // 2 * 2:2]
    slack = jnp.minimum(sizes[giver] - 1, reach - sizes[taker]) // 2
    slack = jnp.where((giver == order[0]) | (taker == order[0]) | (sizes[taker] == 0), 0, jnp.maximum(slack, 0))
    moved = jax.random.randint(jax.random.fold_in(own, 4), (count // 2,), 0, 1 << 20) % (slack + 1)
    sizes = sizes.at[giver].add(-moved).at[taker].add(moved)
    labels = jnp.searchsorted(jnp.cumsum(sizes), jnp.arange(rows * top), side="right").astype(jnp.int32)
    listing = labels.reshape(top, rows).T
    listing = listing[jax.random.permutation(jax.random.fold_in(own, 1), rows)]
    rotation = jax.random.randint(jax.random.fold_in(own, 2), (rows, 1), 0, top)
    return jnp.take_along_axis(listing, (jnp.arange(top)[None, :] + rotation) % top, axis=1)


def load_shares(count, total, bound, lean, full):
    weights = [(1 << 20) // math.isqrt(grade ** lean) + 1 for grade in range(1, count + 1)]
    largest = bound if full else min(bound, max(-(-total // count), total * weights[0] // sum(weights)))
    least = 1 if total - largest >= count - 1 else 0
    holding, surplus = [largest] + [least] * (count - 1), total - largest - least * (count - 1)
    while surplus > 0:
        movable = [i for i in range(1, count) if holding[i] < largest] or [i for i in range(1, count) if holding[i] < bound]
        whole, remaining = sum([weights[i] for i in movable]), surplus
        for i in movable:
            addition = min(bound - holding[i], max(1, remaining * weights[i] // whole), surplus)
            holding[i] = holding[i] + addition
            surplus = surplus - addition
    return np.array(holding)


def noise(rng, shape, spread, bound, split=(), kind=jnp.bfloat16):
    entries = jax.random.normal(rng, shape, jnp.float32) * spread
    if len(split) > 0:
        entries = block_levels(rng, shape, split, -0.22, 0.18) * entries
    return jnp.clip(entries, min=-bound, max=bound).astype(kind)


def setup_inputs(seed: int = 0) -> dict:
    key_of = jax.random.split(jax.random.key(seed), 17)
    hidden = noise(key_of[0], (SEQS, D), 1.0, 6.0, ((0, 128),))
    lengths = plant(jax.random.randint(key_of[1], (SEQS,), 1, CACHE + 1), jax.random.fold_in(key_of[1], 1), 1, CACHE).astype(jnp.int32)
    key_cache = noise(key_of[2], (SEQS, CACHE, KVH * HD), 1.0, 6.0, ((0, 128),))
    value_cache = noise(key_of[3], (SEQS, CACHE, KVH * HD), 1.0, 6.0, ((0, 128),))
    norm_gain = jnp.clip(1.0 + 0.18 * jax.random.normal(key_of[4], (D,), jnp.float32), 0.099609375, 1.8984375).astype(jnp.bfloat16)
    w_query = noise(key_of[5], (D, HEADS * HD), D ** -0.5, 0.125)
    w_key = noise(key_of[6], (D, KVH * HD), D ** -0.5, 0.125)
    w_value = noise(key_of[7], (D, KVH * HD), D ** -0.5, 0.125)
    head_bias = jnp.clip(jax.random.uniform(key_of[8], (HEADS,), jnp.float32, -7.0, -2.0), -7.0, -2.0)
    w_out = noise(key_of[9], (HEADS * HD, D), (HEADS * HD) ** -0.5, 0.1875)
    ffn_gain = jnp.clip(1.0 + 0.18 * jax.random.normal(key_of[10], (D,), jnp.float32), 0.099609375, 1.8984375).astype(jnp.bfloat16)
    routing_keys = jax.random.split(jax.random.fold_in(key_of[11], 1), SEQS // SEQ_DEV)
    routing_turns = jax.random.permutation(jax.random.fold_in(key_of[11], 3), SEQS // SEQ_DEV)
    routing = jax.vmap(lambda own, number: deal_out(jax.random.fold_in(key_of[11], 2), own, number, SEQ_DEV, EXPERTS, TOP, CAP, 1))(routing_keys, routing_turns).reshape((SEQS, TOP))
    route_w = jnp.clip(jnp.exp(math.log(1.0) - 1.6133518 * jax.random.uniform(key_of[12], (SEQS, TOP), jnp.float32) ** block_levels(key_of[12], (SEQS, TOP), ((0, 128),), -0.2, 0.2)), 0.19921875, 1.0).astype(jnp.bfloat16)
    w_gate = noise(key_of[13], (EXPERTS * SLICES, D, FF_DEV), D ** -0.5, 0.125, ((0, 128),))
    w_up = noise(key_of[14], (EXPERTS * SLICES, D, FF_DEV), D ** -0.5, 0.125, ((0, 128),))
    w_down = noise(key_of[15], (EXPERTS * SLICES, FF_DEV, D), FF ** -0.5, 0.078125, ((0, 128),))
    return dict(hidden=hidden, lengths=lengths, key_cache=key_cache, value_cache=value_cache, norm_gain=norm_gain, w_query=w_query, w_key=w_key, w_value=w_value, head_bias=head_bias, w_out=w_out, ffn_gain=ffn_gain, routing=routing, route_w=route_w, w_gate=w_gate, w_up=w_up, w_down=w_down)


def rms_norm(value, gain):
    wide = value.astype(jnp.float32)
    scaled = wide * lax.rsqrt(lax.optimization_barrier(jnp.mean(wide * wide, axis=-1, keepdims=True)) + 1e-06)
    return (scaled * gain.astype(jnp.float32)).astype(jnp.bfloat16)

def attend_block(args):
    query, keys, values, length, bias = args
    count = query.shape[0]
    groups = HEADS // KVH
    q_heads = query.reshape(count, KVH, groups, HD).astype(jnp.float32)
    k_heads = keys.reshape(count, CACHE, KVH, HD).astype(jnp.float32)
    v_heads = values.reshape(count, CACHE, KVH, HD).astype(jnp.float32)
    scores = jnp.einsum('sgrd,scgd->sgrc', q_heads, k_heads) * HD ** (-0.5)
    scores = scores + bias.reshape(KVH, groups)[None, :, :, None]
    mask = (jnp.arange(CACHE, dtype=jnp.int32)[None, :] < length[:, None])[:, None, None, :]
    keep = jnp.where(mask, jax.nn.log_sigmoid(-scores), 0.0)
    after = lax.cumsum(keep, axis=3, reverse=True) - keep
    weight = jnp.where(mask, jnp.exp(jax.nn.log_sigmoid(scores) + after), 0.0).astype(jnp.bfloat16)
    out = jnp.einsum('sgrc,scgd->sgrd', weight.astype(jnp.float32), v_heads)
    return out.reshape(count, HEADS * HD).astype(jnp.bfloat16)

def reference(hidden, lengths, key_cache, value_cache, norm_gain, w_query, w_key, w_value, head_bias, w_out, ffn_gain, routing, route_w, w_gate, w_up, w_down):
    seqs = hidden.shape[0]
    blocks = seqs // SEQ_DEV
    normed = rms_norm(hidden, norm_gain)
    query = jnp.dot(normed, w_query, preferred_element_type=jnp.float32).astype(jnp.bfloat16)
    new_key = jnp.dot(normed, w_key, preferred_element_type=jnp.float32).astype(jnp.bfloat16)
    new_value = jnp.dot(normed, w_value, preferred_element_type=jnp.float32).astype(jnp.bfloat16)
    attended = lax.map(lambda xs: attend_block((xs[0], xs[1], xs[2], xs[3], head_bias)), (query.reshape(blocks, SEQ_DEV, HEADS * HD), key_cache.reshape(blocks, SEQ_DEV, CACHE, KVH * HD), value_cache.reshape(blocks, SEQ_DEV, CACHE, KVH * HD), lengths.reshape(blocks, SEQ_DEV)))
    attended = attended.reshape(seqs, HEADS * HD)
    after_attention = (hidden.astype(jnp.float32) + jnp.dot(attended, w_out, preferred_element_type=jnp.float32)).astype(jnp.bfloat16)
    expert_in = rms_norm(after_attention, ffn_gain)
    slices = w_gate.shape[0] // EXPERTS
    part = w_gate.shape[2]
    gate_all = w_gate.reshape(EXPERTS, slices, D, part)
    up_all = w_up.reshape(EXPERTS, slices, D, part)
    down_all = w_down.reshape(EXPERTS, slices * part, D)
    cap = SEQ_DEV // 2
    slots = blocks * cap
    token_ids = jnp.arange(seqs, dtype=jnp.int32)

    def one_expert(total, expert):
        picked = routing == expert
        named = jnp.any(picked, axis=1).astype(jnp.int32)
        weight = lax.optimization_barrier(jnp.sum(jnp.where(picked, route_w.astype(jnp.float32), 0.0), axis=1))
        rank = jnp.cumsum(named.reshape(blocks, SEQ_DEV), axis=1) - 1
        place = jnp.arange(blocks, dtype=jnp.int32)[:, None] * cap + rank
        place = jnp.where(named.reshape(blocks, SEQ_DEV) > 0, place, slots).reshape(seqs).astype(jnp.int32)
        index = jnp.zeros((slots,), jnp.int32).at[place].set(token_ids, mode='drop')
        valid = jnp.zeros((slots,), jnp.float32).at[place].set(1.0, mode='drop')
        rows = expert_in[index]
        gate_w = jnp.transpose(lax.dynamic_index_in_dim(gate_all, expert, 0, False), (1, 0, 2)).reshape(D, slices * part)
        up_w = jnp.transpose(lax.dynamic_index_in_dim(up_all, expert, 0, False), (1, 0, 2)).reshape(D, slices * part)
        down_w = lax.dynamic_index_in_dim(down_all, expert, 0, False)
        gate = jnp.dot(rows, gate_w, preferred_element_type=jnp.float32)
        upper = jnp.dot(rows, up_w, preferred_element_type=jnp.float32)
        act = (jax.nn.silu(gate) * upper).astype(jnp.bfloat16)
        out = jnp.dot(act, down_w, preferred_element_type=jnp.float32)
        scale = weight[index] * valid
        return (total.at[index].add(out * scale[:, None]), None)
    combined, unused = lax.scan(one_expert, jnp.zeros((seqs, D), jnp.float32), jnp.arange(EXPERTS, dtype=jnp.int32))
    mixed = (after_attention.astype(jnp.float32) + combined).astype(jnp.bfloat16)
    return (mixed, new_key, new_value)
```

```python
import jax
import jax.numpy as jnp
from jax import lax
from jax.experimental import pallas as pl
from jax.experimental.pallas import tpu as pltpu
from jax.sharding import PartitionSpec as P

D = 2048
HEADS = 16
HD = 64
CACHE = 1024
SEQ = 8
FFD = 352
HALF = D // 2
F32 = jnp.float32
BF16 = jnp.bfloat16
MESH = pl.DeviceIdType.MESH
XOFF = (0, 3, 1, 2)
GROUPS = (0, 1, 3, 2)
QCHUNK = 4
OCHUNK = 2


def rms_norm(wide, gain):
    scaled = wide * lax.rsqrt(jnp.mean(wide * wide, axis=-1, keepdims=True) + 1e-06)
    return (scaled * gain).astype(BF16)


def kernel(
    hidden_ref, lengths_ref, key_hbm, value_hbm, norm_gain_ref, wq_hbm, wk_hbm, wv_hbm, bias_ref,
    wo_hbm, ffn_gain_ref, routing_ref, route_w_ref, wg_hbm, wu_hbm, wd_hbm,
    mixed_ref, newk_ref, newv_ref,
    wq, wk, wv, kc, vc, wo, wg, wu, wd,
    qs, zs, kp, osc, table, xin, xsend, msg, blk, pblk, ofull, obuf, pout, rbuf, ybuf, fsend, fbuf,
    lsem, tsend, trecv, xs_sem, xr_sem, d1s, d1r, ringp_s, ringp_r, ringm_s, ringm_r, rel_s, rel_r,
    ps, pr, os_, orr, ys, yr, fs, fr,
):
    me = lax.axis_index("ep")
    c = me % 2
    x = (me // 2) % 4
    y = (me // 8) % 4
    z = me // 32

    def dev(dz, dy, dx, core):
        return ((((z + dz) % 4) * 4 + (y + dy) % 4) * 4 + (x + dx) % 4) * 2 + core

    def remote(src, dst, ssem, rsem, target):
        return pltpu.make_async_remote_copy(
            src_ref=src, dst_ref=dst, send_sem=ssem, recv_sem=rsem,
            device_id=(target,), device_id_type=MESH,
        )

    def drain(ref, sem):
        pltpu.make_async_copy(ref, ref, sem).wait()

    loads = {}

    def load(name, src, dst):
        copy = pltpu.make_async_copy(src, dst, lsem.at[len(loads)])
        copy.start()
        loads[name] = copy

    qrows = D // QCHUNK
    for i in range(QCHUNK):
        load(("wq", i), wq_hbm.at[pl.ds(i * qrows, qrows)], wq.at[pl.ds(i * qrows, qrows)])
    load("key", key_hbm, kc)
    load("value", value_hbm, vc)
    orows = HEADS * HD // OCHUNK
    for i in range(OCHUNK):
        load(("wo", i), wo_hbm.at[pl.ds(i * orows, orows)], wo.at[pl.ds(i * orows, orows)])
    load("wk", wk_hbm, wk)
    load("wv", wv_hbm, wv)
    for i in range(2):
        half = (c + i) % 2
        load(("wg", i), wg_hbm.at[0, pl.ds(half * HALF, HALF)], wg.at[i])
        load(("wu", i), wu_hbm.at[0, pl.ds(half * HALF, HALF)], wu.at[i])
    for i in range(2):
        half = (c + i) % 2
        load(("wd", i), wd_hbm.at[0, :, pl.ds(pl.multiple_of(half * HALF, HALF), HALF)], wd.at[i])

    barrier = pltpu.get_barrier_semaphore()
    partners = [dev(d // 4, d % 4, 0, c) for d in range(1, 16)]
    row = [(k, core) for k in range(4) for core in range(2)]
    rowdev = [(k, o) for k in range(4) for o in range(2) if k + o > 0]
    partners += [dev(0, 0, 4 - XOFF[k], (c + o) % 2) for k, o in rowdev]
    for target in partners:
        pl.semaphore_signal(barrier, inc=1, device_id=(target,), device_id_type=MESH)

    lane = lax.broadcasted_iota(jnp.int32, (SEQ, 128), 1)
    plane = lane // 8
    lz = (z + plane // 4) % 4
    ly = (y + plane % 4) % 4
    lexpert = 2 * lz + ly // 2
    first, second = routing_ref[:, 0:1], routing_ref[:, 1:2]
    route_w = route_w_ref[...].astype(F32)
    is_first, is_second = lexpert == first, lexpert == second
    named = jnp.where(is_first | is_second, 1.0, 0.0).astype(F32)
    tri = (
        lax.broadcasted_iota(jnp.int32, (SEQ, SEQ), 0) >= lax.broadcasted_iota(jnp.int32, (SEQ, SEQ), 1)
    ).astype(F32)
    rank = jnp.dot(tri, named, preferred_element_type=F32)
    here = (jnp.abs(rank - 1.0 - (lane % 4).astype(F32)) < 0.5) & ((lane // 4) % 2 == c)
    weight = jnp.where(is_first, route_w[:, 0:1], jnp.where(is_second, route_w[:, 1:2], 0.0))
    table[0, c] = jnp.where(here, weight, 0.0)

    hidden = hidden_ref[...].astype(F32)
    normed = rms_norm(hidden, norm_gain_ref[...].astype(F32).reshape(1, D))
    query = jnp.zeros((SEQ, HEADS * HD), F32)
    for i in range(QCHUNK):
        loads[("wq", i)].wait()
        query = query + jnp.dot(
            normed[:, i * qrows : (i + 1) * qrows], wq[i * qrows : (i + 1) * qrows, :],
            preferred_element_type=F32,
        )
    query = query.astype(BF16).astype(F32)
    low = lax.broadcasted_iota(jnp.int32, (SEQ, 128), 1) < HD
    for j in range(8):
        tile = query[:, j * 128 : (j + 1) * 128]
        swapped = pltpu.roll(tile, HD, 1)
        if j < 4:
            even, odd = jnp.where(low, tile, 0.0), jnp.where(low, swapped, 0.0)
        else:
            even, odd = jnp.where(low, 0.0, swapped), jnp.where(low, 0.0, tile)
        qs[pl.ds(16 * j, 8), :] = even
        qs[pl.ds(16 * j + 8, 8), :] = odd

    pl.semaphore_wait(barrier, len(partners))
    tcopies = []
    for i, (k, o) in enumerate(rowdev):
        copy = remote(
            table.at[0, c], table.at[k, c], tsend.at[i], trecv.at[i],
            dev(0, 0, 4 - XOFF[k], (c + o) % 2),
        )
        copy.start()
        tcopies.append(copy)

    loads["key"].wait()
    sub = lax.broadcasted_iota(jnp.int32, (HEADS, 128), 0)
    bias = jnp.zeros((HEADS, 128), F32)
    for h in range(HEADS):
        bias = jnp.where(sub == h, bias_ref[h], bias)
    bias = jnp.concatenate([bias] * 8, axis=1)
    position = lax.broadcasted_iota(jnp.int32, (HEADS, CACHE), 1)
    for s in range(SEQ):
        q = qs[pl.ds(s, HEADS, stride=SEQ), :].astype(BF16)
        scores = lax.dot_general(
            q, kc[s], (((1,), (1,)), ((), ())), preferred_element_type=F32
        ) * (HD ** -0.5) + bias
        soft = jnp.log(1.0 + jnp.exp(-jnp.abs(scores)))
        used = position < lengths_ref[s]
        keep = jnp.where(used, -(jnp.maximum(scores, 0.0) + soft), 0.0)
        zs[s] = jnp.where(used, jnp.minimum(scores, 0.0) - soft, -1e30)
        high = keep.astype(BF16)
        rest = (keep - high.astype(F32)).astype(BF16)
        for b in range(4):
            kp[0, s, b] = high[:, b * 256 : (b + 1) * 256]
            kp[1, s, b] = rest[:, b * 256 : (b + 1) * 256]
    col = lax.broadcasted_iota(jnp.int32, (256, 384), 1)
    below = (lax.broadcasted_iota(jnp.int32, (256, 384), 0) > col) | (col >= 256)
    below = jnp.where(below, 1.0, 0.0).astype(BF16)
    loads["value"].wait()
    for s in range(SEQ):
        sums = jnp.dot(kp[0, s].reshape(64, 256), below, preferred_element_type=F32)
        sums = sums + jnp.dot(kp[1, s].reshape(64, 256), below, preferred_element_type=F32)
        carry = jnp.zeros((HEADS, 128), F32)
        parts = [None] * 4
        for b in (3, 2, 1, 0):
            piece = sums[b * 16 : (b + 1) * 16]
            after = piece[:, :256] + jnp.concatenate([carry, carry], axis=1)
            parts[b] = jnp.exp(zs[s, :, b * 256 : (b + 1) * 256] + after).astype(BF16)
            carry = carry + piece[:, 256:]
        weights = jnp.concatenate(parts, axis=1)
        out = jnp.dot(weights, vc[s], preferred_element_type=F32)
        osc[pl.ds(s, HEADS, stride=SEQ), :] = out
    pieces = []
    for j in range(8):
        even, odd = osc[pl.ds(16 * j, 8), :], osc[pl.ds(16 * j + 8, 8), :]
        if j < 4:
            pieces.append(jnp.where(low, even, pltpu.roll(odd, HD, 1)))
        else:
            pieces.append(jnp.where(low, pltpu.roll(even, HD, 1), odd))
    attended = jnp.concatenate(pieces, axis=1).astype(BF16)
    after = hidden
    for i in range(OCHUNK):
        loads[("wo", i)].wait()
        after = after + jnp.dot(
            attended[:, i * orows : (i + 1) * orows], wo[i * orows : (i + 1) * orows, :],
            preferred_element_type=F32,
        )
    after = after.astype(BF16).astype(F32)
    expert_in = rms_norm(after, ffn_gain_ref[...].astype(F32).reshape(1, D)).astype(F32)

    mine = jnp.where(c == 0, expert_in[:, :HALF], expert_in[:, HALF:])
    xin[c] = mine
    xsend[...] = jnp.where(c == 0, expert_in[:, HALF:], expert_in[:, :HALF])
    swap = remote(xsend, xin.at[c], xs_sem, xr_sem, dev(0, 0, 0, 1 - c))
    swap.start()

    loads["wk"].wait()
    loads["wv"].wait()
    newk_ref[...] = jnp.dot(normed, wk[...], preferred_element_type=F32).astype(BF16)
    newv_ref[...] = jnp.dot(normed, wv[...], preferred_element_type=F32).astype(BF16)
    for copy in tcopies:
        copy.wait()

    swap.wait()
    places = jnp.where(table[0].reshape(16, 128) > 0.0, 1.0, 0.0).astype(BF16)
    tokens = xin[...].reshape(16, HALF).astype(BF16)
    packed = lax.dot_general(
        places, tokens, (((0,), (0,)), ((), ())), preferred_element_type=F32
    ).reshape(16, 8, HALF).astype(BF16)
    msg[...] = packed
    blk[0, 0] = packed[0]
    for d in (1, 2, 3, 4, 5, 6, 7, 12, 13, 14, 15, 8, 9, 10, 11):
        remote(
            msg.at[d], blk.at[0, d], d1s, d1r.at[d // 4], dev(d // 4, d % 4, 0, c)
        ).start()

    def rows(g):
        return pl.ds(4 * g, 4)

    def share(k, g):
        copy = remote(blk.at[k, rows(g)], pblk.at[k, rows(g)], ps.at[k, g], pr.at[k, g], dev(0, 0, 0, 1 - c))
        copy.start()
        return copy

    plus, minus, shared, relays = {}, {}, {}, {}
    for g in GROUPS:
        start = 4 * g + (1 if g == 0 else 0)
        drain(blk.at[0, pl.ds(start, 4 * g + 4 - start)], d1r.at[g])
        plus[g] = remote(blk.at[0, rows(g)], blk.at[1, rows(g)], ringp_s.at[g], ringp_r.at[g], dev(0, 0, 1, c))
        plus[g].start()
        minus[g] = remote(blk.at[0, rows(g)], blk.at[2, rows(g)], ringm_s.at[g], ringm_r.at[g], dev(0, 0, 3, c))
        minus[g].start()
        shared[0, g] = share(0, g)

    for name in [("wg", 0), ("wg", 1), ("wu", 0), ("wu", 1), ("wd", 0), ("wd", 1)]:
        loads[name].wait()

    def take(g):
        plus[g].wait_recv()
        shared[1, g] = share(1, g)
        if g in (0, 3):
            relays[g] = remote(blk.at[1, rows(g)], blk.at[3, rows(g)], rel_s.at[g], rel_r.at[g], dev(0, 0, 1, c))
            relays[g].start()
        minus[g].wait_recv()
        shared[2, g] = share(2, g)
        if g in (1, 2):
            relays[g] = remote(blk.at[2, rows(g)], blk.at[3, rows(g)], rel_s.at[g], rel_r.at[g], dev(0, 0, 3, c))
            relays[g].start()

    oshare = {}

    def experts(k):
        for g in GROUPS:
            shared[k, g].wait_recv()
        own, other = blk[k].reshape(128, HALF), pblk[k].reshape(128, HALF)
        gate = jnp.dot(own, wg[0], preferred_element_type=F32) + jnp.dot(other, wg[1], preferred_element_type=F32)
        upper = jnp.dot(own, wu[0], preferred_element_type=F32) + jnp.dot(other, wu[1], preferred_element_type=F32)
        act = (jax.nn.silu(gate) * upper).astype(BF16)
        obuf[k] = jnp.dot(act, wd[1], preferred_element_type=F32).reshape(16, 8, HALF).astype(BF16)
        oshare[k] = remote(obuf.at[k], pout.at[k], os_.at[k], orr.at[k], dev(0, 0, 0, 1 - c))
        oshare[k].start()
        ofull[k] = jnp.dot(act, wd[0], preferred_element_type=F32).reshape(16, 8, HALF)

    def give_back(k):
        oshare[k].wait_recv()
        total = (ofull[k] + pout[k].astype(F32)).astype(BF16)
        rbuf[k] = total
        ybuf[k, 0] = total[0]
        for d in range(1, 16):
            remote(
                rbuf.at[k, d], ybuf.at[k, d], ys.at[k], yr.at[k], dev(4 - d // 4, 4 - d % 4, 0, c)
            ).start()

    take(0)
    experts(0)
    give_back(0)
    take(1)
    take(3)
    take(2)
    experts(1)
    experts(2)
    give_back(1)
    for g in GROUPS:
        relays[g].wait_recv()
        shared[3, g] = share(3, g)
    give_back(2)
    experts(3)
    give_back(3)

    fcopies = []
    for k in range(4):
        drain(ybuf.at[k, pl.ds(1, 15)], yr.at[k])
        scale = table[k].reshape(16, 128).astype(BF16)
        combined = jnp.dot(scale, ybuf[k].reshape(128, HALF), preferred_element_type=F32)
        combined = combined.reshape(2, SEQ, HALF).astype(BF16)
        fsend[k] = combined
        for o in range(2):
            core = (c + o) % 2
            if k == 0 and o == 0:
                fbuf[0, c] = fsend[0, c]
                continue
            copy = remote(
                fsend.at[k, core], fbuf.at[k, c], fs.at[k, o], fr.at[k, o], dev(0, 0, XOFF[k], core)
            )
            copy.start()
            fcopies.append(copy)
    for copy in fcopies:
        copy.wait()
    total = fbuf[0].astype(F32) + fbuf[1].astype(F32) + fbuf[2].astype(F32) + fbuf[3].astype(F32)
    mixed_ref[:, :HALF] = (after[:, :HALF] + total[0]).astype(BF16)
    mixed_ref[:, HALF:] = (after[:, HALF:] + total[1]).astype(BF16)

    drain(msg.at[pl.ds(1, 15)], d1s)
    for g in range(4):
        plus[g].wait_send()
        minus[g].wait_send()
        relays[g].wait_send()
        for k in range(4):
            shared[k, g].wait_send()
    for k in range(4):
        oshare[k].wait_send()
        drain(rbuf.at[k, pl.ds(1, 15)], ys.at[k])


def local(*args):
    vmem = pl.BlockSpec(memory_space=pltpu.VMEM)
    smem = pl.BlockSpec(memory_space=pltpu.SMEM)
    hbm = pl.BlockSpec(memory_space=pl.ANY)
    dma = pltpu.SemaphoreType.DMA
    scratch = [
        pltpu.VMEM((D, HEADS * HD), BF16),
        pltpu.VMEM((D, 128), BF16),
        pltpu.VMEM((D, 128), BF16),
        pltpu.VMEM((SEQ, CACHE, 128), BF16),
        pltpu.VMEM((SEQ, CACHE, 128), BF16),
        pltpu.VMEM((HEADS * HD, D), BF16),
        pltpu.VMEM((2, HALF, FFD), BF16),
        pltpu.VMEM((2, HALF, FFD), BF16),
        pltpu.VMEM((2, FFD, HALF), BF16),
        pltpu.VMEM((128, 128), F32),
        pltpu.VMEM((SEQ, HEADS, CACHE), F32),
        pltpu.VMEM((2, SEQ, 4, HEADS, 256), BF16),
        pltpu.VMEM((128, 128), F32),
        pltpu.VMEM((4, 2, SEQ, 128), F32),
        pltpu.VMEM((2, SEQ, HALF), F32),
        pltpu.VMEM((SEQ, HALF), F32),
        pltpu.VMEM((16, 8, HALF), BF16),
        pltpu.VMEM((4, 16, 8, HALF), BF16),
        pltpu.VMEM((4, 16, 8, HALF), BF16),
        pltpu.VMEM((4, 16, 8, HALF), F32),
        pltpu.VMEM((4, 16, 8, HALF), BF16),
        pltpu.VMEM((4, 16, 8, HALF), BF16),
        pltpu.VMEM((4, 16, 8, HALF), BF16),
        pltpu.VMEM((4, 16, 8, HALF), BF16),
        pltpu.VMEM((4, 2, SEQ, HALF), BF16),
        pltpu.VMEM((4, 2, SEQ, HALF), BF16),
        dma((QCHUNK + OCHUNK + 10,)),
        dma((7,)), dma((7,)),
        dma, dma,
        dma, dma((4,)),
        dma((4,)), dma((4,)),
        dma((4,)), dma((4,)),
        dma((4,)), dma((4,)),
        dma((4, 4)), dma((4, 4)),
        dma((4,)), dma((4,)),
        dma((4,)), dma((4,)),
        dma((4, 2)), dma((4, 2)),
    ]
    return pl.pallas_call(
        kernel,
        out_shape=(
            jax.ShapeDtypeStruct((SEQ, D), BF16),
            jax.ShapeDtypeStruct((SEQ, 128), BF16),
            jax.ShapeDtypeStruct((SEQ, 128), BF16),
        ),
        in_specs=[vmem, smem, hbm, hbm, vmem, hbm, hbm, hbm, smem, hbm, vmem, vmem, vmem, hbm, hbm, hbm],
        out_specs=(vmem, vmem, vmem),
        scratch_shapes=scratch,
        compiler_params=pltpu.CompilerParams(
            collective_id=0, has_side_effects=True, vmem_limit_bytes=60 * 2**20
        ),
        name="layer",
    )(*args)


def solution(mesh):
    ep2, ep3 = P("ep", None), P("ep", None, None)
    in_specs = (ep2, P("ep"), ep3, ep3, P(), P(), P(), P(), P(), P(), P(), ep2, ep2, ep3, ep3, ep3)
    return jax.shard_map(
        local, mesh=mesh, in_specs=in_specs, out_specs=(ep2, ep2, ep2), check_vma=False
    )
```

```python
import jax
import jax.numpy as jnp
from jax import lax
from jax.experimental import pallas as pl
from jax.experimental.pallas import tpu as pltpu
from jax.sharding import PartitionSpec as P

D = 2048
HEADS = 16
HD = 64
CACHE = 1024
SEQ = 8
FFD = 352
HALF = D // 2
F32 = jnp.float32
BF16 = jnp.bfloat16
MESH = pl.DeviceIdType.MESH
XOFF = (0, 3, 1, 2)
GROUPS = (0, 1, 3, 2)
QCHUNK = 4
OCHUNK = 2


def rms_norm(wide, gain):
    scaled = wide * lax.rsqrt(jnp.mean(wide * wide, axis=-1, keepdims=True) + 1e-06)
    return (scaled * gain).astype(BF16)


def dot_t(a, b):
    return lax.dot_general(a, b, (((1,), (1,)), ((), ())), preferred_element_type=F32)


def kernel(
    hidden_hbm, lengths_ref, key_hbm, value_hbm, norm_gain_hbm, wq_hbm, wk_hbm, wv_hbm, bias_ref,
    wo_hbm, ffn_gain_hbm, routing_hbm, route_w_hbm, wg_hbm, wu_hbm, wd_hbm,
    mixed_hbm, newk_hbm, newv_hbm,
    hidden_ref, norm_gain_ref, ffn_gain_ref, routing_ref, route_w_ref, mixed_ref, newk_ref, newv_ref,
    wq, wkv, kc, vc, wo, wexp,
    qs, zs, kp, sums, osc, table, xin, xsend, msg, blk, pblk, ofull, obuf, pout, rbuf, ybuf, fsend, fbuf,
    lsem, kvsem, esem, tsend, trecv, xs_sem, xr_sem, d1s, d1r, ring_s, ringp_r, ringm_r, rel_s, rel_r,
    ps, pr, os_, orr, ys, yr, fs, fr, outs,
):
    me = lax.axis_index("ep")
    c = me % 2
    x = (me // 2) % 4
    y = (me // 8) % 4
    z = me // 32

    def dev(dz, dy, dx, core):
        return ((((z + dz) % 4) * 4 + (y + dy) % 4) * 4 + (x + dx) % 4) * 2 + core

    def remote(src, dst, ssem, rsem, target):
        return pltpu.make_async_remote_copy(
            src_ref=src, dst_ref=dst, send_sem=ssem, recv_sem=rsem,
            device_id=(target,), device_id_type=MESH,
        )

    def drain(ref, sem):
        pltpu.make_async_copy(ref, ref, sem).wait()

    loads = {}

    def load(name, src, dst, shared=None):
        copy = pltpu.make_async_copy(src, dst, lsem.at[len(loads)] if shared is None else shared)
        copy.start()
        if shared is None:
            loads[name] = copy

    load("hidden", hidden_hbm, hidden_ref)
    load("norm_gain", norm_gain_hbm, norm_gain_ref)
    qrows = D // QCHUNK
    for i in range(QCHUNK):
        load(("wq", i), wq_hbm.at[pl.ds(i * qrows, qrows)], wq.at[pl.ds(i * qrows, qrows)])
    load("key", key_hbm, kc)
    load("value", value_hbm, vc)
    load("routing", routing_hbm, routing_ref)
    load("route_w", route_w_hbm, route_w_ref)
    load("ffn_gain", ffn_gain_hbm, ffn_gain_ref)
    orows = HEADS * HD // OCHUNK
    for i in range(OCHUNK):
        load(("wo", i), wo_hbm.at[pl.ds(i * orows, orows)], wo.at[pl.ds(i * orows, orows)])
    load("wk", wk_hbm, wkv.at[0], kvsem)
    load("wv", wv_hbm, wkv.at[1], kvsem)
    barrier = pltpu.get_barrier_semaphore()
    partners = [dev(d // 4, d % 4, 0, c) for d in range(1, 16)]
    row = [(k, core) for k in range(4) for core in range(2)]
    rowdev = [(k, o) for k in range(4) for o in range(2) if k + o > 0]
    partners += [dev(0, 0, 4 - XOFF[k], (c + o) % 2) for k, o in rowdev]
    for target in partners:
        pl.semaphore_signal(barrier, inc=1, device_id=(target,), device_id_type=MESH)

    loads["hidden"].wait()
    loads["norm_gain"].wait()
    hidden = hidden_ref[...].astype(F32)
    normed = rms_norm(hidden, norm_gain_ref[...].astype(F32).reshape(1, D))
    query = jnp.zeros((SEQ, HEADS * HD), F32)
    for i in range(QCHUNK):
        loads[("wq", i)].wait()
        query = query + jnp.dot(
            normed[:, i * qrows : (i + 1) * qrows], wq[i * qrows : (i + 1) * qrows, :],
            preferred_element_type=F32,
        )
    query = query.astype(BF16).astype(F32)
    low = lax.broadcasted_iota(jnp.int32, (SEQ, 128), 1) < HD
    for j in range(8):
        tile = query[:, j * 128 : (j + 1) * 128]
        swapped = pltpu.roll(tile, HD, 1)
        if j < 4:
            even, odd = jnp.where(low, tile, 0.0), jnp.where(low, swapped, 0.0)
        else:
            even, odd = jnp.where(low, 0.0, swapped), jnp.where(low, 0.0, tile)
        qs[pl.ds(16 * j, 8), :] = even
        qs[pl.ds(16 * j + 8, 8), :] = odd

    loads["key"].wait()
    sub = lax.broadcasted_iota(jnp.int32, (HEADS, 128), 0)
    bias = jnp.zeros((HEADS, 128), F32)
    for h in range(HEADS):
        bias = jnp.where(sub == h, bias_ref[h], bias)
    bias = jnp.concatenate([bias] * 8, axis=1)
    position = lax.broadcasted_iota(jnp.int32, (HEADS, CACHE), 1)
    for s in range(SEQ):
        q = qs[pl.ds(s, HEADS, stride=SEQ), :].astype(BF16)
        scores = lax.dot_general(
            q, kc[s], (((1,), (1,)), ((), ())), preferred_element_type=F32
        ) * (HD ** -0.5) + bias
        soft = jnp.log(1.0 + jnp.exp(-jnp.abs(scores)))
        used = position < lengths_ref[s]
        keep = jnp.where(used, -(jnp.maximum(scores, 0.0) + soft), 0.0)
        zs[s] = jnp.where(used, jnp.minimum(scores, 0.0) - soft, -1e30)
        high = keep.astype(BF16)
        rest = (keep - high.astype(F32)).astype(BF16)
        for b in range(4):
            kp[s, b, :, :256] = high[:, b * 256 : (b + 1) * 256]
            kp[s, b, :, 256:] = rest[:, b * 256 : (b + 1) * 256]
    col = lax.broadcasted_iota(jnp.int32, (512, 384), 1)
    below = (lax.broadcasted_iota(jnp.int32, (512, 384), 0) % 256 > col) | (col >= 256)
    below = jnp.where(below, 1.0, 0.0).astype(BF16)
    sums[...] = jnp.dot(kp[...].reshape(512, 512), below, preferred_element_type=F32)
    loads["value"].wait()
    for s in range(SEQ):
        carry = jnp.zeros((HEADS, 128), F32)
        parts = [None] * 4
        for b in (3, 2, 1, 0):
            piece = sums[pl.ds(s * 64 + b * 16, 16), :]
            after = piece[:, :256] + jnp.concatenate([carry, carry], axis=1)
            parts[b] = jnp.exp(zs[s, :, b * 256 : (b + 1) * 256] + after).astype(BF16)
            carry = carry + piece[:, 256:]
        weights = jnp.concatenate(parts, axis=1)
        out = jnp.dot(weights, vc[s], preferred_element_type=F32)
        osc[pl.ds(s, HEADS, stride=SEQ), :] = out
    pieces = []
    for j in range(8):
        even, odd = osc[pl.ds(16 * j, 8), :], osc[pl.ds(16 * j + 8, 8), :]
        if j < 4:
            pieces.append(jnp.where(low, even, pltpu.roll(odd, HD, 1)))
        else:
            pieces.append(jnp.where(low, pltpu.roll(even, HD, 1), odd))
    attended = jnp.concatenate(pieces, axis=1).astype(BF16)
    after = hidden
    for i in range(OCHUNK):
        loads[("wo", i)].wait()
        after = after + jnp.dot(
            attended[:, i * orows : (i + 1) * orows], wo[i * orows : (i + 1) * orows, :],
            preferred_element_type=F32,
        )
    after = after.astype(BF16).astype(F32)
    loads["ffn_gain"].wait()
    expert_in = rms_norm(after, ffn_gain_ref[...].astype(F32).reshape(1, D)).astype(F32)

    for i in range(2):
        half = (c + i) % 2
        cols = pl.ds(pl.multiple_of(half * HALF, HALF), HALF)
        load("wg", wg_hbm.at[0, :, cols], wexp.at[i], esem)
        load("wu", wu_hbm.at[0, :, cols], wexp.at[2 + i], esem)
        load("wd", wd_hbm.at[0, :, cols], wexp.at[4 + i], esem)

    lane = lax.broadcasted_iota(jnp.int32, (SEQ, 128), 1)
    plane = lane // 8
    lz = (z + plane // 4) % 4
    ly = (y + plane % 4) % 4
    lexpert = 2 * lz + ly // 2
    diagonal = lax.broadcasted_iota(jnp.int32, (SEQ, SEQ), 0) == lax.broadcasted_iota(jnp.int32, (SEQ, SEQ), 1)

    def column(row):
        return jnp.sum(jnp.where(diagonal, row, 0.0), axis=1, keepdims=True)

    loads["routing"].wait()
    loads["route_w"].wait()
    routing = routing_ref[...].astype(F32)
    route_w = route_w_ref[...].astype(F32)
    lexpert = lexpert.astype(F32)
    is_first = jnp.abs(lexpert - column(routing[0:1])) < 0.5
    is_second = jnp.abs(lexpert - column(routing[1:2])) < 0.5
    named = jnp.where(is_first | is_second, 1.0, 0.0).astype(F32)
    tri = (
        lax.broadcasted_iota(jnp.int32, (SEQ, SEQ), 0) >= lax.broadcasted_iota(jnp.int32, (SEQ, SEQ), 1)
    ).astype(F32)
    rank = jnp.dot(tri, named, preferred_element_type=F32)
    here = (jnp.abs(rank - 1.0 - (lane % 4).astype(F32)) < 0.5) & ((lane // 4) % 2 == c)
    weight = jnp.where(is_first, column(route_w[0:1]), jnp.where(is_second, column(route_w[1:2]), 0.0))
    table[c] = jnp.where(here, weight, 0.0)

    pl.semaphore_wait(barrier, len(partners))
    for i, (k, o) in enumerate(rowdev):
        copy = remote(
            table.at[c], table.at[2 * k + c], tsend, trecv.at[min(k, 1)],
            dev(0, 0, 4 - XOFF[k], (c + o) % 2),
        )
        copy.start()

    mine = jnp.where(c == 0, expert_in[:, :HALF], expert_in[:, HALF:])
    xin[c] = mine
    xsend[...] = jnp.where(c == 0, expert_in[:, HALF:], expert_in[:, :HALF])
    swap = remote(xsend, xin.at[c], xs_sem, xr_sem, dev(0, 0, 0, 1 - c))
    swap.start()

    drain(wkv, kvsem)
    newk_ref[...] = jnp.dot(normed, wkv[0], preferred_element_type=F32).astype(BF16)
    newv_ref[...] = jnp.dot(normed, wkv[1], preferred_element_type=F32).astype(BF16)
    out_copies = [
        pltpu.make_async_copy(newk_ref, newk_hbm, outs.at[0]),
        pltpu.make_async_copy(newv_ref, newv_hbm, outs.at[1]),
    ]
    for copy in out_copies:
        copy.start()
    drain(table.at[0], trecv.at[0])

    swap.wait_recv()
    places = jnp.where(table[0:2].reshape(16, 128) > 0.0, 1.0, 0.0).astype(BF16)
    tokens = xin[...].reshape(16, HALF).astype(BF16)
    packed = lax.dot_general(
        places, tokens, (((0,), (0,)), ((), ())), preferred_element_type=F32
    ).reshape(16, 8, HALF).astype(BF16)
    msg[...] = packed
    blk[0, 0] = packed[0]
    for d in (1, 2, 3, 4, 5, 6, 7, 12, 13, 14, 15, 8, 9, 10, 11):
        remote(
            msg.at[d], blk.at[0, d], d1s, d1r.at[d // 4], dev(d // 4, d % 4, 0, c)
        ).start()

    def rows(g):
        return pl.ds(4 * g, 4)

    def share(k, g):
        copy = remote(blk.at[k, rows(g)], pblk.at[k, rows(g)], ps, pr.at[k], dev(0, 0, 0, 1 - c))
        copy.start()

    plus, minus, relays = {}, {}, {}
    for g in GROUPS:
        start = 4 * g + (1 if g == 0 else 0)
        drain(blk.at[0, pl.ds(start, 4 * g + 4 - start)], d1r.at[g])
        plus[g] = remote(blk.at[0, rows(g)], blk.at[1, rows(g)], ring_s, ringp_r.at[g], dev(0, 0, 1, c))
        plus[g].start()
        minus[g] = remote(blk.at[0, rows(g)], blk.at[2, rows(g)], ring_s, ringm_r.at[g], dev(0, 0, 3, c))
        minus[g].start()
        share(0, g)

    drain(wexp, esem)

    def take(g):
        plus[g].wait_recv()
        share(1, g)
        if g in (0, 3):
            relays[g] = remote(blk.at[1, rows(g)], blk.at[3, rows(g)], rel_s, rel_r.at[g], dev(0, 0, 1, c))
            relays[g].start()
        minus[g].wait_recv()
        share(2, g)
        if g in (1, 2):
            relays[g] = remote(blk.at[2, rows(g)], blk.at[3, rows(g)], rel_s, rel_r.at[g], dev(0, 0, 3, c))
            relays[g].start()

    oshare = {}

    def experts(k, count):
        span = pl.ds(k, count)
        own = blk[span].reshape(128 * count, HALF)
        gate, upper = dot_t(wexp[0], own), dot_t(wexp[2], own)
        for j in range(k, k + count):
            drain(pblk.at[j], pr.at[j])
        other = pblk[span].reshape(128 * count, HALF)
        gate, upper = gate + dot_t(wexp[1], other), upper + dot_t(wexp[3], other)
        act = (jax.nn.silu(gate) * upper).T.astype(BF16)
        theirs = jnp.dot(act, wexp[5], preferred_element_type=F32)
        obuf[span] = theirs.reshape(count, 16, 8, HALF).astype(BF16)
        for j in range(k, k + count):
            oshare[j] = remote(obuf.at[j], pout.at[j], os_, orr.at[j], dev(0, 0, 0, 1 - c))
            oshare[j].start()
        ofull[span] = jnp.dot(act, wexp[4], preferred_element_type=F32).reshape(count, 16, 8, HALF)

    def give_back(k):
        oshare[k].wait_recv()
        total = (ofull[k] + pout[k].astype(F32)).astype(BF16)
        rbuf[k] = total
        ybuf[k, 0] = total[0]
        for d in (10, 9, 11, 6, 14, 8, 2, 5, 7, 13, 15, 4, 12, 1, 3):
            remote(
                rbuf.at[k, d], ybuf.at[k, d], ys, yr.at[k], dev(4 - d // 4, 4 - d % 4, 0, c)
            ).start()

    take(0)
    experts(0, 1)
    take(1)
    give_back(0)
    take(3)
    take(2)
    experts(1, 2)
    for g in GROUPS:
        relays[g].wait_recv()
        share(3, g)
    give_back(1)
    give_back(2)
    experts(3, 1)
    give_back(3)

    drain(table.at[pl.ds(2, 6)], trecv.at[1])
    for k in range(4):
        drain(ybuf.at[k, pl.ds(1, 15)], yr.at[k])
        scale = table[2 * k : 2 * k + 2].reshape(16, 128).astype(BF16)
        combined = jnp.dot(scale, ybuf[k].reshape(128, HALF), preferred_element_type=F32)
        combined = combined.reshape(2, SEQ, HALF).astype(BF16)
        for core in range(2):
            fsend[2 * k + core] = combined[core]
        for o in range(2):
            core = (c + o) % 2
            if k == 0 and o == 0:
                fbuf[0, c] = jnp.where(c == 0, combined[0], combined[1])
                continue
            remote(
                fsend.at[2 * k + core], fbuf.at[k, c], fs, fr, dev(0, 0, XOFF[k], core)
            ).start()
    drain(fsend.at[pl.ds(0, 7)], fr)
    total = fbuf[0].astype(F32) + fbuf[1].astype(F32) + fbuf[2].astype(F32) + fbuf[3].astype(F32)
    mixed_ref[:, :HALF] = (after[:, :HALF] + total[0]).astype(BF16)
    mixed_ref[:, HALF:] = (after[:, HALF:] + total[1]).astype(BF16)
    out_copies.append(pltpu.make_async_copy(mixed_ref, mixed_hbm, outs.at[2]))
    out_copies[-1].start()

    drain(fsend.at[pl.ds(0, 7)], fs)
    drain(table.at[pl.ds(0, 7)], tsend)
    swap.wait_send()
    drain(msg.at[pl.ds(1, 15)], d1s)
    drain(blk.at[pl.ds(0, 2)], ring_s)
    drain(blk.at[0], rel_s)
    drain(blk, ps)
    drain(obuf, os_)
    drain(rbuf.at[:, pl.ds(1, 15)], ys)
    for copy in out_copies:
        copy.wait()


def finish(mixed_in, newk_in, newv_in, mixed_ref, newk_ref, newv_ref):
    mixed_ref[...] = mixed_in[...]
    newk_ref[...] = newk_in[...]
    newv_ref[...] = newv_in[...]


def local(*args):
    args = list(args)
    args[11], args[12] = args[11].T, args[12].T
    args[13], args[14] = jnp.swapaxes(args[13], 1, 2), jnp.swapaxes(args[14], 1, 2)
    vmem = pl.BlockSpec(memory_space=pltpu.VMEM)
    smem = pl.BlockSpec(memory_space=pltpu.SMEM)
    hbm = pl.BlockSpec(memory_space=pl.ANY)
    dma = pltpu.SemaphoreType.DMA
    scratch = [
        pltpu.VMEM((SEQ, D), BF16),
        pltpu.VMEM((D,), BF16),
        pltpu.VMEM((D,), BF16),
        pltpu.VMEM((2, SEQ), jnp.int32),
        pltpu.VMEM((2, SEQ), BF16),
        pltpu.VMEM((SEQ, D), BF16),
        pltpu.VMEM((SEQ, 128), BF16),
        pltpu.VMEM((SEQ, 128), BF16),
        pltpu.VMEM((D, HEADS * HD), BF16),
        pltpu.VMEM((2, D, 128), BF16),
        pltpu.VMEM((SEQ, CACHE, 128), BF16),
        pltpu.VMEM((SEQ, CACHE, 128), BF16),
        pltpu.VMEM((HEADS * HD, D), BF16),
        pltpu.VMEM((6, FFD, HALF), BF16),
        pltpu.VMEM((128, 128), F32),
        pltpu.VMEM((SEQ, HEADS, CACHE), F32),
        pltpu.VMEM((SEQ, 4, HEADS, 512), BF16),
        pltpu.VMEM((512, 384), F32),
        pltpu.VMEM((128, 128), F32),
        pltpu.VMEM((8, SEQ, 128), F32),
        pltpu.VMEM((2, SEQ, HALF), F32),
        pltpu.VMEM((SEQ, HALF), F32),
        pltpu.VMEM((16, 8, HALF), BF16),
        pltpu.VMEM((4, 16, 8, HALF), BF16),
        pltpu.VMEM((4, 16, 8, HALF), BF16),
        pltpu.VMEM((4, 16, 8, HALF), F32),
        pltpu.VMEM((4, 16, 8, HALF), BF16),
        pltpu.VMEM((4, 16, 8, HALF), BF16),
        pltpu.VMEM((4, 16, 8, HALF), BF16),
        pltpu.VMEM((4, 16, 8, HALF), BF16),
        pltpu.VMEM((8, SEQ, HALF), BF16),
        pltpu.VMEM((4, 2, SEQ, HALF), BF16),
        dma((QCHUNK + OCHUNK + 7,)), dma, dma,
        dma, dma((2,)),
        dma, dma,
        dma, dma((4,)),
        dma, dma((4,)), dma((4,)),
        dma, dma((4,)),
        dma, dma((4,)),
        dma, dma((4,)),
        dma, dma((4,)),
        dma, dma,
        dma((3,)),
    ]
    out_shape = (
        jax.ShapeDtypeStruct((SEQ, D), BF16),
        jax.ShapeDtypeStruct((SEQ, 128), BF16),
        jax.ShapeDtypeStruct((SEQ, 128), BF16),
    )
    outs = pl.pallas_call(
        kernel,
        out_shape=out_shape,
        in_specs=[hbm, smem, hbm, hbm, hbm, hbm, hbm, hbm, smem, hbm, hbm, hbm, hbm, hbm, hbm, hbm],
        out_specs=(hbm, hbm, hbm),
        scratch_shapes=scratch,
        compiler_params=pltpu.CompilerParams(
            collective_id=0, has_side_effects=True, vmem_limit_bytes=60 * 2**20
        ),
        name="layer",
    )(*args)
    return pl.pallas_call(
        finish, out_shape=out_shape, in_specs=[vmem] * 3, out_specs=(vmem,) * 3, name="finish"
    )(*outs)


def solution(mesh):
    ep2, ep3 = P("ep", None), P("ep", None, None)
    in_specs = (ep2, P("ep"), ep3, ep3, P(), P(), P(), P(), P(), P(), P(), ep2, ep2, ep3, ep3, ep3)
    return jax.shard_map(
        local, mesh=mesh, in_specs=in_specs, out_specs=(ep2, ep2, ep2), check_vma=False
    )
```

```python
import jax
import jax.numpy as jnp
from jax import lax
from jax.experimental import pallas as pl
from jax.experimental.pallas import tpu as pltpu
from jax.sharding import PartitionSpec as P

D = 2048
HEADS = 16
HD = 64
CACHE = 1024
SEQ = 8
FFD = 352
HALF = D // 2
QUART = HALF // 2
F32 = jnp.float32
BF16 = jnp.bfloat16
MESH = pl.DeviceIdType.MESH
XOFF = (0, 2, 3, 1)
GROUPS = (0, 1, 3, 2)
QCHUNK = 4
OCHUNK = 2


def rms_norm(wide, gain):
    scaled = wide * lax.rsqrt(jnp.mean(wide * wide, axis=-1, keepdims=True) + 1e-06)
    return (scaled * gain).astype(BF16)


def dot_t(a, b):
    return lax.dot_general(a, b, (((1,), (1,)), ((), ())), preferred_element_type=F32)


def kernel(
    hidden_hbm, lengths_ref, key_hbm, value_hbm, norm_gain_hbm, wq_hbm, wk_hbm, wv_hbm, bias_ref,
    wo_hbm, ffn_gain_hbm, routing_hbm, route_w_hbm, wg_hbm, wu_hbm, wd_hbm,
    mixed_ref, newk_ref, newv_ref,
    hidden_ref, norm_gain_ref, ffn_gain_ref, routing_ref, route_w_ref,
    wq, wkv, kc, vc, wo, wexp,
    qs, zs, kp, sums, osc, table, xin, xsend, xfar, msg, msgfar, blk, pblk, ofull, obuf, pout, rbuf, ghold, gbuf, gmsg, ybuf, fsend, fbuf,
    lsem, kvsem, esem, tsend, trecv, xs_sem, xr_sem, xf_s, xf_r, d1s, d1r, d3s, d3r, ring_s, ringp_r, ringm_r,
    ps, pr, os_, orr, ys, yls, yr, gs, gr, ygs, ygr, fs, fr, fls, flr, fgs, fgr,
):
    me = lax.axis_index("ep")
    c = me % 2
    x = (me // 2) % 4
    y = (me // 8) % 4
    z = me // 32

    def dev(dz, dy, dx, core):
        return ((((z + dz) % 4) * 4 + (y + dy) % 4) * 4 + (x + dx) % 4) * 2 + core

    def remote(src, dst, ssem, rsem, target):
        return pltpu.make_async_remote_copy(
            src_ref=src, dst_ref=dst, send_sem=ssem, recv_sem=rsem,
            device_id=(target,), device_id_type=MESH,
        )

    def drain(ref, sem):
        pltpu.make_async_copy(ref, ref, sem).wait()

    loads = {}

    def load(name, src, dst, shared=None):
        copy = pltpu.make_async_copy(src, dst, lsem.at[len(loads)] if shared is None else shared)
        copy.start()
        if shared is None:
            loads[name] = copy

    load("hidden", hidden_hbm, hidden_ref)
    load("norm_gain", norm_gain_hbm, norm_gain_ref)
    load("routing", routing_hbm, routing_ref)
    load("route_w", route_w_hbm, route_w_ref)
    load("ffn_gain", ffn_gain_hbm, ffn_gain_ref)
    qrows = D // QCHUNK
    for i in range(QCHUNK):
        load(("wq", i), wq_hbm.at[pl.ds(i * qrows, qrows)], wq.at[pl.ds(i * qrows, qrows)])
    load("key", key_hbm, kc)
    load("value", value_hbm, vc)
    orows = HEADS * HD // OCHUNK
    for i in range(OCHUNK):
        load(("wo", i), wo_hbm.at[pl.ds(i * orows, orows)], wo.at[pl.ds(i * orows, orows)])
    load("wk", wk_hbm, wkv.at[0], kvsem)
    load("wv", wv_hbm, wkv.at[1], kvsem)
    barrier = pltpu.get_barrier_semaphore()
    partners = [dev(d // 4, d % 4, 0, c) for d in range(1, 16)]
    row = [(k, core) for k in range(4) for core in range(2)]
    rowdev = [(k, o) for k in range(4) for o in range(2) if k + o > 0]
    partners += [dev(0, 0, 4 - XOFF[k], (c + o) % 2) for k, o in rowdev]
    for target in partners:
        pl.semaphore_signal(barrier, inc=1, device_id=(target,), device_id_type=MESH)

    loads["hidden"].wait()
    loads["norm_gain"].wait()
    hidden = hidden_ref[...].astype(F32)
    normed = rms_norm(hidden, norm_gain_ref[...].astype(F32).reshape(1, D))
    query = jnp.zeros((SEQ, HEADS * HD), F32)
    for i in range(QCHUNK):
        loads[("wq", i)].wait()
        query = query + jnp.dot(
            normed[:, i * qrows : (i + 1) * qrows], wq[i * qrows : (i + 1) * qrows, :],
            preferred_element_type=F32,
        )
    query = query.astype(BF16).astype(F32)
    low = lax.broadcasted_iota(jnp.int32, (SEQ, 128), 1) < HD
    for j in range(8):
        tile = query[:, j * 128 : (j + 1) * 128]
        swapped = pltpu.roll(tile, HD, 1)
        if j < 4:
            even, odd = jnp.where(low, tile, 0.0), jnp.where(low, swapped, 0.0)
        else:
            even, odd = jnp.where(low, 0.0, swapped), jnp.where(low, 0.0, tile)
        qs[pl.ds(16 * j, 8), :] = even
        qs[pl.ds(16 * j + 8, 8), :] = odd

    lane = lax.broadcasted_iota(jnp.int32, (SEQ, 128), 1)
    plane = lane // 8
    lz = (z + plane // 4) % 4
    ly = (y + plane % 4) % 4
    lexpert = 2 * lz + ly // 2
    diagonal = lax.broadcasted_iota(jnp.int32, (SEQ, SEQ), 0) == lax.broadcasted_iota(jnp.int32, (SEQ, SEQ), 1)

    def column(row):
        return jnp.sum(jnp.where(diagonal, row, 0.0), axis=1, keepdims=True)

    loads["routing"].wait()
    loads["route_w"].wait()
    routing = routing_ref[...].astype(F32)
    route_w = route_w_ref[...].astype(F32)
    lexpert = lexpert.astype(F32)
    is_first = jnp.abs(lexpert - column(routing[0:1])) < 0.5
    is_second = jnp.abs(lexpert - column(routing[1:2])) < 0.5
    named = jnp.where(is_first | is_second, 1.0, 0.0).astype(F32)
    tri = (
        lax.broadcasted_iota(jnp.int32, (SEQ, SEQ), 0) >= lax.broadcasted_iota(jnp.int32, (SEQ, SEQ), 1)
    ).astype(F32)
    rank = jnp.dot(tri, named, preferred_element_type=F32)
    here = (jnp.abs(rank - 1.0 - (lane % 4).astype(F32)) < 0.5) & ((lane // 4) % 2 == c)
    weight = jnp.where(is_first, column(route_w[0:1]), jnp.where(is_second, column(route_w[1:2]), 0.0))
    table[c] = jnp.where(here, weight, 0.0)

    loads["key"].wait()
    sub = lax.broadcasted_iota(jnp.int32, (HEADS, 128), 0)
    bias = jnp.zeros((HEADS, 128), F32)
    for h in range(HEADS):
        bias = jnp.where(sub == h, bias_ref[h], bias)
    bias = jnp.concatenate([bias] * 8, axis=1)
    position = lax.broadcasted_iota(jnp.int32, (HEADS, CACHE), 1)
    for s in range(SEQ):
        q = qs[pl.ds(s, HEADS, stride=SEQ), :].astype(BF16)
        scores = lax.dot_general(
            q, kc[s], (((1,), (1,)), ((), ())), preferred_element_type=F32
        ) * (HD ** -0.5) + bias
        soft = jnp.log(1.0 + jnp.exp(-jnp.abs(scores)))
        used = position < lengths_ref[s]
        keep = jnp.where(used, -(jnp.maximum(scores, 0.0) + soft), 0.0)
        zs[s] = jnp.where(used, jnp.minimum(scores, 0.0) - soft, -1e30)
        high = keep.astype(BF16)
        rest = (keep - high.astype(F32)).astype(BF16)
        for b in range(4):
            kp[s, b, :, :256] = high[:, b * 256 : (b + 1) * 256]
            kp[s, b, :, 256:] = rest[:, b * 256 : (b + 1) * 256]
    col = lax.broadcasted_iota(jnp.int32, (512, 384), 1)
    below = (lax.broadcasted_iota(jnp.int32, (512, 384), 0) % 256 > col) | (col >= 256)
    below = jnp.where(below, 1.0, 0.0).astype(BF16)
    sums[...] = jnp.dot(kp[...].reshape(512, 512), below, preferred_element_type=F32)
    loads["value"].wait()
    for s in range(SEQ):
        carry = jnp.zeros((HEADS, 128), F32)
        parts = [None] * 4
        for b in (3, 2, 1, 0):
            piece = sums[pl.ds(s * 64 + b * 16, 16), :]
            after = piece[:, :256] + jnp.concatenate([carry, carry], axis=1)
            parts[b] = jnp.exp(zs[s, :, b * 256 : (b + 1) * 256] + after).astype(BF16)
            carry = carry + piece[:, 256:]
        weights = jnp.concatenate(parts, axis=1)
        out = jnp.dot(weights, vc[s], preferred_element_type=F32)
        osc[pl.ds(s, HEADS, stride=SEQ), :] = out
    pieces = []
    for j in range(8):
        even, odd = osc[pl.ds(16 * j, 8), :], osc[pl.ds(16 * j + 8, 8), :]
        if j < 4:
            pieces.append(jnp.where(low, even, pltpu.roll(odd, HD, 1)))
        else:
            pieces.append(jnp.where(low, pltpu.roll(even, HD, 1), odd))
    attended = jnp.concatenate(pieces, axis=1).astype(BF16)
    after = hidden
    for i in range(OCHUNK):
        loads[("wo", i)].wait()
        after = after + jnp.dot(
            attended[:, i * orows : (i + 1) * orows], wo[i * orows : (i + 1) * orows, :],
            preferred_element_type=F32,
        )
    after = after.astype(BF16).astype(F32)
    loads["ffn_gain"].wait()
    expert_in = rms_norm(after, ffn_gain_ref[...].astype(F32).reshape(1, D)).astype(F32)

    for i in range(2):
        half = (c + i) % 2
        cols = pl.ds(pl.multiple_of(half * HALF, HALF), HALF)
        load("wg", wg_hbm.at[0, :, cols], wexp.at[i], esem)
        load("wu", wu_hbm.at[0, :, cols], wexp.at[2 + i], esem)
        load("wd", wd_hbm.at[0, :, cols], wexp.at[4 + i], esem)

    pl.semaphore_wait(barrier, len(partners))
    for i, (k, o) in enumerate(rowdev):
        copy = remote(
            table.at[c], table.at[2 * k + c], tsend, trecv.at[(0, 2, 1, 1)[k]],
            dev(0, 0, 4 - XOFF[k], (c + o) % 2),
        )
        copy.start()

    mine = jnp.where(c == 0, expert_in[:, :HALF], expert_in[:, HALF:])
    xin[c] = mine.astype(BF16)
    xsend[...] = jnp.where(c == 0, expert_in[:, HALF:], expert_in[:, :HALF]).astype(BF16)
    swap = remote(xsend, xin.at[c], xs_sem, xr_sem, dev(0, 0, 0, 1 - c))
    swap.start()
    far = [
        remote(xin.at[c], xfar.at[c], xf_s.at[0], xf_r.at[0], dev(0, 0, 2, c)),
        remote(xsend, xfar.at[c], xf_s.at[1], xf_r.at[1], dev(0, 0, 2, 1 - c)),
    ]
    for copy in far:
        copy.start()

    drain(wkv, kvsem)
    newk_ref[...] = jnp.dot(normed, wkv[0], preferred_element_type=F32).astype(BF16)
    newv_ref[...] = jnp.dot(normed, wkv[1], preferred_element_type=F32).astype(BF16)
    drain(table.at[0], trecv.at[0])

    swap.wait_recv()

    def dispatch(k, tokens_ref, out, ssem, rsem):
        places = jnp.where(table[2 * k : 2 * k + 2].reshape(16, 128) > 0.0, 1.0, 0.0).astype(BF16)
        tokens = tokens_ref[...].astype(F32).reshape(16, HALF).astype(BF16)
        packed = lax.dot_general(
            places, tokens, (((0,), (0,)), ((), ())), preferred_element_type=F32
        ).reshape(16, 8, HALF).astype(BF16)
        out[...] = packed
        blk[k, 0] = packed[0]
        for d in (1, 2, 3, 4, 5, 6, 7, 12, 13, 14, 15, 8, 9, 10, 11):
            remote(
                out.at[d], blk.at[k, d], ssem, rsem.at[d // 4], dev(d // 4, d % 4, 0, c)
            ).start()

    dispatch(0, xin, msg, d1s, d1r)
    drain(table.at[pl.ds(0, 2)], trecv.at[2])
    for copy in far:
        copy.wait_recv()
    dispatch(1, xfar, msgfar, d3s, d3r)

    def rows(g):
        return pl.ds(4 * g, 4)

    def share(k, g):
        copy = remote(blk.at[k, rows(g)], pblk.at[k, rows(g)], ps, pr.at[k], dev(0, 0, 0, 1 - c))
        copy.start()

    plus, minus = {}, {}
    def arrive(k, g, sem):
        start = 4 * g + (1 if g == 0 else 0)
        drain(blk.at[k, pl.ds(start, 4 * g + 4 - start)], sem.at[g])

    for g in GROUPS:
        arrive(0, g, d1r)
        plus[g] = remote(blk.at[0, rows(g)], blk.at[2, rows(g)], ring_s, ringp_r.at[g], dev(0, 0, 1, c))
        plus[g].start()
        minus[g] = remote(blk.at[0, rows(g)], blk.at[3, rows(g)], ring_s, ringm_r.at[g], dev(0, 0, 3, c))
        minus[g].start()
        share(0, g)

    drain(wexp, esem)

    def take(g):
        plus[g].wait_recv()
        share(2, g)
        minus[g].wait_recv()
        share(3, g)

    def take_far(g):
        arrive(1, g, d3r)
        share(1, g)

    oshare = {}

    def experts(k, count):
        span = pl.ds(k, count)
        own = blk[span].reshape(128 * count, HALF)
        gate, upper = dot_t(wexp[0], own), dot_t(wexp[2], own)
        for j in range(k, k + count):
            drain(pblk.at[j], pr.at[j])
        other = pblk[span].reshape(128 * count, HALF)
        gate, upper = gate + dot_t(wexp[1], other), upper + dot_t(wexp[3], other)
        act = (jax.nn.silu(gate) * upper).T.astype(BF16)
        theirs = jnp.dot(act, wexp[5], preferred_element_type=F32)
        obuf[span] = theirs.reshape(count, 16, 8, HALF).astype(BF16)
        for j in range(k, k + count):
            oshare[j] = remote(obuf.at[j], pout.at[j], os_, orr.at[j], dev(0, 0, 0, 1 - c))
            oshare[j].start()
        ofull[span] = jnp.dot(act, wexp[4], preferred_element_type=F32).reshape(count, 16, 8, HALF)

    spread = (10, 9, 11, 6, 14, 8, 2, 5, 7, 13, 15, 4, 12, 1, 3)
    left, right = pl.ds(0, QUART), pl.ds(QUART, QUART)

    def give_back(k):
        oshare[k].wait_recv()
        total = ofull[k] + pout[k].astype(F32)
        rounded = total.astype(BF16)
        rbuf[k] = rounded
        if k == 1:
            ybuf[k, 0] = rounded[0]
            for d in spread:
                remote(
                    rbuf.at[k, d], ybuf.at[k, d], ys, yr.at[k], dev(4 - d // 4, 4 - d % 4, 0, c)
                ).start()
            return
        if k > 0:
            for h in (1, 0):
                part = pl.ds(8 * h, 8)
                remote(
                    rbuf.at[k, part, :, right], gbuf.at[k - 2, part], gs, gr.at[h], dev(0, 0, XOFF[k], c)
                ).start()
        else:
            ghold[...] = total[:, :, QUART:]
        ybuf[k, 0, :, :QUART] = rounded[0, :, :QUART]
        for d in spread:
            remote(
                rbuf.at[k, d, :, left], ybuf.at[k, d, :, left], yls, yr.at[k],
                dev(4 - d // 4, 4 - d % 4, 0, c),
            ).start()

    def merge(h):
        part = pl.ds(8 * h, 8)
        drain(gbuf.at[:, part], gr.at[h])
        total = ghold[part] + gbuf[0, part].astype(F32) + gbuf[1, part].astype(F32)
        gmsg[part] = total.astype(BF16)
        if h == 0:
            ybuf[0, 0, :, QUART:] = total[0].astype(BF16)
        for d in spread:
            if d // 8 == h:
                remote(
                    gmsg.at[d], ybuf.at[0, d, :, right], ygs, ygr, dev(4 - d // 4, 4 - d % 4, 0, c)
                ).start()

    take_far(0)
    take_far(1)
    take(0)
    take_far(3)
    take_far(2)
    take(1)
    experts(0, 2)
    take(3)
    take(2)
    give_back(0)
    give_back(1)
    experts(2, 2)
    give_back(2)
    give_back(3)
    merge(1)
    merge(0)

    drain(table.at[pl.ds(4, 4)], trecv.at[1])
    def combine(k, low, high):
        scale = table[2 * k : 2 * k + 2].reshape(16, 128).astype(BF16)
        sums = jnp.dot(scale, ybuf[k, :, :, low:high].reshape(128, high - low), preferred_element_type=F32)
        return sums.reshape(2, SEQ, high - low).astype(BF16)

    def deliver(k, o, send, recv, cols):
        core = (c + o) % 2
        remote(
            fsend.at[2 * k + core, :, cols], fbuf.at[k, c, :, cols], send, recv, dev(0, 0, XOFF[k], core)
        ).start()

    for k in (0, 1, 2, 3):
        if k == 1:
            drain(ybuf.at[1, pl.ds(1, 15)], yr.at[1])
            fsend[2:4] = combine(1, 0, HALF)
            deliver(1, 0, fs, fr, pl.ds(0, HALF))
            deliver(1, 1, fs, fr, pl.ds(0, HALF))
            continue
        drain(ybuf.at[k, pl.ds(1, 15), :, left], yr.at[k])
        fsend[2 * k : 2 * k + 2, :, :QUART] = combine(k, 0, QUART)
        for o in range(2):
            if k + o > 0:
                deliver(k, o, fls, flr, left)
    drain(ybuf.at[0, pl.ds(1, 15), :, right], ygr)
    fsend[0:2, :, QUART:] = combine(0, QUART, HALF)
    deliver(0, 1, fgs, fgr, right)
    fbuf[0, c] = fsend[c]
    drain(fsend.at[pl.ds(0, 5), :, left], flr)
    drain(fsend.at[pl.ds(0, 2)], fr)
    drain(fsend.at[0, :, right], fgr)
    low = fbuf[0, :, :, :QUART].astype(F32) + fbuf[3, :, :, :QUART].astype(F32)
    low = low + fbuf[1, :, :, :QUART].astype(F32) + fbuf[2, :, :, :QUART].astype(F32)
    high = fbuf[0, :, :, QUART:].astype(F32) + fbuf[1, :, :, QUART:].astype(F32)
    total = jnp.concatenate([low, high], axis=-1)
    mixed_ref[:, :HALF] = (after[:, :HALF] + total[0]).astype(BF16)
    mixed_ref[:, HALF:] = (after[:, HALF:] + total[1]).astype(BF16)

    drain(fsend.at[pl.ds(0, 5), :, left], fls)
    drain(fsend.at[pl.ds(0, 2)], fs)
    drain(fsend.at[0, :, right], fgs)
    drain(rbuf.at[pl.ds(2, 2), :, :, right], gs)
    drain(rbuf.at[pl.ds(0, 3), pl.ds(1, 15), :, left], yls)
    drain(gmsg.at[pl.ds(1, 15)], ygs)
    drain(table.at[pl.ds(0, 7)], tsend)
    swap.wait_send()
    for copy in far:
        copy.wait_send()
    drain(msg.at[pl.ds(1, 15)], d1s)
    drain(blk.at[pl.ds(0, 2)], ring_s)
    drain(msgfar.at[pl.ds(1, 15)], d3s)
    drain(blk, ps)
    drain(obuf, os_)
    drain(rbuf.at[1, pl.ds(1, 15)], ys)


def finish(mixed_in, newk_in, newv_in, mixed_ref, newk_ref, newv_ref):
    mixed_ref[...] = mixed_in[...]
    newk_ref[...] = newk_in[...]
    newv_ref[...] = newv_in[...]


def local(*args):
    args = list(args)
    args[11], args[12] = args[11].T, args[12].T
    args[13], args[14] = jnp.swapaxes(args[13], 1, 2), jnp.swapaxes(args[14], 1, 2)
    vmem = pl.BlockSpec(memory_space=pltpu.VMEM)
    smem = pl.BlockSpec(memory_space=pltpu.SMEM)
    hbm = pl.BlockSpec(memory_space=pl.ANY)
    dma = pltpu.SemaphoreType.DMA
    scratch = [
        pltpu.VMEM((SEQ, D), BF16),
        pltpu.VMEM((D,), BF16),
        pltpu.VMEM((D,), BF16),
        pltpu.VMEM((2, SEQ), jnp.int32),
        pltpu.VMEM((2, SEQ), BF16),
        pltpu.VMEM((D, HEADS * HD), BF16),
        pltpu.VMEM((2, D, 128), BF16),
        pltpu.VMEM((SEQ, CACHE, 128), BF16),
        pltpu.VMEM((SEQ, CACHE, 128), BF16),
        pltpu.VMEM((HEADS * HD, D), BF16),
        pltpu.VMEM((6, FFD, HALF), BF16),
        pltpu.VMEM((128, 128), F32),
        pltpu.VMEM((SEQ, HEADS, CACHE), F32),
        pltpu.VMEM((SEQ, 4, HEADS, 512), BF16),
        pltpu.VMEM((512, 384), F32),
        pltpu.VMEM((128, 128), F32),
        pltpu.VMEM((8, SEQ, 128), F32),
        pltpu.VMEM((2, SEQ, HALF), BF16),
        pltpu.VMEM((SEQ, HALF), BF16),
        pltpu.VMEM((2, SEQ, HALF), BF16),
        pltpu.VMEM((16, 8, HALF), BF16),
        pltpu.VMEM((16, 8, HALF), BF16),
        pltpu.VMEM((4, 16, 8, HALF), BF16),
        pltpu.VMEM((4, 16, 8, HALF), BF16),
        pltpu.VMEM((4, 16, 8, HALF), F32),
        pltpu.VMEM((4, 16, 8, HALF), BF16),
        pltpu.VMEM((4, 16, 8, HALF), BF16),
        pltpu.VMEM((4, 16, 8, HALF), BF16),
        pltpu.VMEM((16, 8, QUART), F32),
        pltpu.VMEM((2, 16, 8, QUART), BF16),
        pltpu.VMEM((16, 8, QUART), BF16),
        pltpu.VMEM((4, 16, 8, HALF), BF16),
        pltpu.VMEM((8, SEQ, HALF), BF16),
        pltpu.VMEM((4, 2, SEQ, HALF), BF16),
        dma((QCHUNK + OCHUNK + 7,)), dma, dma,
        dma, dma((3,)),
        dma, dma,
        dma((2,)), dma((2,)),
        dma, dma((4,)),
        dma, dma((4,)),
        dma, dma((4,)), dma((4,)),
        dma, dma((4,)),
        dma, dma((4,)),
        dma, dma, dma((4,)),
        dma, dma((2,)),
        dma, dma,
        dma, dma, dma, dma, dma, dma,
    ]
    out_shape = (
        jax.ShapeDtypeStruct((SEQ, D), BF16),
        jax.ShapeDtypeStruct((SEQ, 128), BF16),
        jax.ShapeDtypeStruct((SEQ, 128), BF16),
    )
    outs = pl.pallas_call(
        kernel,
        out_shape=tuple(pltpu.VMEM(o.shape, o.dtype) for o in out_shape),
        in_specs=[hbm, smem, hbm, hbm, hbm, hbm, hbm, hbm, smem, hbm, hbm, hbm, hbm, hbm, hbm, hbm],
        out_specs=(vmem, vmem, vmem),
        scratch_shapes=scratch,
        compiler_params=pltpu.CompilerParams(
            collective_id=0, has_side_effects=True, vmem_limit_bytes=60 * 2**20
        ),
        name="layer",
    )(*args)
    return pl.pallas_call(
        finish, out_shape=out_shape, in_specs=[vmem] * 3, out_specs=(vmem,) * 3, name="finish"
    )(*[pltpu.with_memory_space_constraint(o, pltpu.VMEM) for o in outs])


def solution(mesh):
    ep2, ep3 = P("ep", None), P("ep", None, None)
    in_specs = (ep2, P("ep"), ep3, ep3, P(), P(), P(), P(), P(), P(), P(), ep2, ep2, ep3, ep3, ep3)
    return jax.shard_map(
        local, mesh=mesh, in_specs=in_specs, out_specs=(ep2, ep2, ep2), check_vma=False
    )
```

```python
import jax
import jax.numpy as jnp
from jax import lax
from jax.experimental import pallas as pl
from jax.experimental.pallas import tpu as pltpu
from jax.sharding import PartitionSpec as P

D = 2048
HEADS = 16
HD = 64
CACHE = 1024
SEQ = 8
FFD = 352
HALF = D // 2
LEFT = 512
RIGHT = HALF - LEFT
F32 = jnp.float32
BF16 = jnp.bfloat16
MESH = pl.DeviceIdType.MESH
XOFF = (0, 2, 3, 1)
GROUPS = (0, 1, 3, 2)
QCHUNK = 4
OCHUNK = 2


def rms_norm(wide, gain):
    scaled = wide * lax.rsqrt(jnp.mean(wide * wide, axis=-1, keepdims=True) + 1e-06)
    return (scaled * gain).astype(BF16)


def dot_t(a, b):
    return lax.dot_general(a, b, (((1,), (1,)), ((), ())), preferred_element_type=F32)


def kernel(
    hidden_hbm, lengths_ref, key_hbm, value_hbm, norm_gain_hbm, wq_hbm, wk_hbm, wv_hbm, bias_ref,
    wo_hbm, ffn_gain_hbm, routing_hbm, route_w_hbm, wg_hbm, wu_hbm, wd_hbm,
    mixed_ref, newk_ref, newv_ref,
    hidden_ref, norm_gain_ref, ffn_gain_ref, routing_ref, route_w_ref,
    wq, wkv, kc, vc, wo, wexp,
    qs, zs, kp, sums, osc, table, xin, xsend, xfar, msg, msgfar, blk, pblk, ofull, obuf, pout, rbuf, ghold, gbuf, gmsg, ybuf, fsend, fbuf,
    lsem, kvsem, esem, tsend, trecv, xs_sem, xr_sem, xf_s, xf_r, d1s, d1r, d3s, d3r, ring_s, ringp_r, ringm_r,
    ps, pr, os_, orr, orh, ys, yls, yr, gs, gr, ygs, ygr, fs, fr, fls, flr, fgs, fgr,
):
    me = lax.axis_index("ep")
    c = me % 2
    x = (me // 2) % 4
    y = (me // 8) % 4
    z = me // 32

    def dev(dz, dy, dx, core):
        return ((((z + dz) % 4) * 4 + (y + dy) % 4) * 4 + (x + dx) % 4) * 2 + core

    def remote(src, dst, ssem, rsem, target):
        return pltpu.make_async_remote_copy(
            src_ref=src, dst_ref=dst, send_sem=ssem, recv_sem=rsem,
            device_id=(target,), device_id_type=MESH,
        )

    def drain(ref, sem):
        pltpu.make_async_copy(ref, ref, sem).wait()

    loads = {}

    def load(name, src, dst, shared=None):
        copy = pltpu.make_async_copy(src, dst, lsem.at[len(loads)] if shared is None else shared)
        copy.start()
        if shared is None:
            loads[name] = copy

    load("hidden", hidden_hbm, hidden_ref)
    load("norm_gain", norm_gain_hbm, norm_gain_ref)
    load("routing", routing_hbm, routing_ref)
    load("route_w", route_w_hbm, route_w_ref)
    load("ffn_gain", ffn_gain_hbm, ffn_gain_ref)
    qrows = D // QCHUNK
    for i in range(QCHUNK):
        load(("wq", i), wq_hbm.at[pl.ds(i * qrows, qrows)], wq.at[pl.ds(i * qrows, qrows)])
    load("key", key_hbm, kc)
    load("value", value_hbm, vc)
    orows = HEADS * HD // OCHUNK
    for i in range(OCHUNK):
        load(("wo", i), wo_hbm.at[pl.ds(i * orows, orows)], wo.at[pl.ds(i * orows, orows)])
    load("wk", wk_hbm, wkv.at[0], kvsem)
    load("wv", wv_hbm, wkv.at[1], kvsem)
    barrier = pltpu.get_barrier_semaphore()
    partners = [dev(d // 4, d % 4, 0, c) for d in range(1, 16)]
    row = [(k, core) for k in range(4) for core in range(2)]
    rowdev = [(k, o) for k in range(4) for o in range(2) if k + o > 0]
    partners += [dev(0, 0, 4 - XOFF[k], (c + o) % 2) for k, o in rowdev]
    for target in partners:
        pl.semaphore_signal(barrier, inc=1, device_id=(target,), device_id_type=MESH)

    loads["hidden"].wait()
    loads["norm_gain"].wait()
    hidden = hidden_ref[...].astype(F32)
    normed = rms_norm(hidden, norm_gain_ref[...].astype(F32).reshape(1, D))
    query = jnp.zeros((SEQ, HEADS * HD), F32)
    for i in range(QCHUNK):
        loads[("wq", i)].wait()
        query = query + jnp.dot(
            normed[:, i * qrows : (i + 1) * qrows], wq[i * qrows : (i + 1) * qrows, :],
            preferred_element_type=F32,
        )
    query = query.astype(BF16).astype(F32)
    low = lax.broadcasted_iota(jnp.int32, (SEQ, 128), 1) < HD
    for j in range(8):
        tile = query[:, j * 128 : (j + 1) * 128]
        swapped = pltpu.roll(tile, HD, 1)
        if j < 4:
            even, odd = jnp.where(low, tile, 0.0), jnp.where(low, swapped, 0.0)
        else:
            even, odd = jnp.where(low, 0.0, swapped), jnp.where(low, 0.0, tile)
        qs[pl.ds(16 * j, 8), :] = even
        qs[pl.ds(16 * j + 8, 8), :] = odd

    lane = lax.broadcasted_iota(jnp.int32, (SEQ, 128), 1)
    plane = lane // 8
    lz = (z + plane // 4) % 4
    ly = (y + plane % 4) % 4
    lexpert = 2 * lz + ly // 2
    diagonal = lax.broadcasted_iota(jnp.int32, (SEQ, SEQ), 0) == lax.broadcasted_iota(jnp.int32, (SEQ, SEQ), 1)

    def column(row):
        return jnp.sum(jnp.where(diagonal, row, 0.0), axis=1, keepdims=True)

    loads["routing"].wait()
    loads["route_w"].wait()
    routing = routing_ref[...].astype(F32)
    route_w = route_w_ref[...].astype(F32)
    lexpert = lexpert.astype(F32)
    is_first = jnp.abs(lexpert - column(routing[0:1])) < 0.5
    is_second = jnp.abs(lexpert - column(routing[1:2])) < 0.5
    named = jnp.where(is_first | is_second, 1.0, 0.0).astype(F32)
    tri = (
        lax.broadcasted_iota(jnp.int32, (SEQ, SEQ), 0) >= lax.broadcasted_iota(jnp.int32, (SEQ, SEQ), 1)
    ).astype(F32)
    rank = jnp.dot(tri, named, preferred_element_type=F32)
    here = (jnp.abs(rank - 1.0 - (lane % 4).astype(F32)) < 0.5) & ((lane // 4) % 2 == c)
    weight = jnp.where(is_first, column(route_w[0:1]), jnp.where(is_second, column(route_w[1:2]), 0.0))
    table[c] = jnp.where(here, weight, 0.0)

    loads["key"].wait()
    sub = lax.broadcasted_iota(jnp.int32, (HEADS, 128), 0)
    bias = jnp.zeros((HEADS, 128), F32)
    for h in range(HEADS):
        bias = jnp.where(sub == h, bias_ref[h], bias)
    bias = jnp.concatenate([bias] * 8, axis=1)
    position = lax.broadcasted_iota(jnp.int32, (HEADS, CACHE), 1)
    for s in range(SEQ):
        q = qs[pl.ds(s, HEADS, stride=SEQ), :].astype(BF16)
        scores = lax.dot_general(
            q, kc[s], (((1,), (1,)), ((), ())), preferred_element_type=F32
        ) * (HD ** -0.5) + bias
        soft = jnp.log(1.0 + jnp.exp(-jnp.abs(scores)))
        used = position < lengths_ref[s]
        keep = jnp.where(used, -(jnp.maximum(scores, 0.0) + soft), 0.0)
        zs[s] = jnp.where(used, jnp.minimum(scores, 0.0) - soft, -1e30)
        high = keep.astype(BF16)
        rest = (keep - high.astype(F32)).astype(BF16)
        for b in range(4):
            kp[s, b, :, :256] = high[:, b * 256 : (b + 1) * 256]
            kp[s, b, :, 256:] = rest[:, b * 256 : (b + 1) * 256]
    col = lax.broadcasted_iota(jnp.int32, (512, 384), 1)
    below = (lax.broadcasted_iota(jnp.int32, (512, 384), 0) % 256 > col) | (col >= 256)
    below = jnp.where(below, 1.0, 0.0).astype(BF16)
    sums[...] = jnp.dot(kp[...].reshape(512, 512), below, preferred_element_type=F32)
    loads["value"].wait()
    for s in range(SEQ):
        carry = jnp.zeros((HEADS, 128), F32)
        parts = [None] * 4
        for b in (3, 2, 1, 0):
            piece = sums[pl.ds(s * 64 + b * 16, 16), :]
            after = piece[:, :256] + jnp.concatenate([carry, carry], axis=1)
            parts[b] = jnp.exp(zs[s, :, b * 256 : (b + 1) * 256] + after).astype(BF16)
            carry = carry + piece[:, 256:]
        weights = jnp.concatenate(parts, axis=1)
        out = jnp.dot(weights, vc[s], preferred_element_type=F32)
        osc[pl.ds(s, HEADS, stride=SEQ), :] = out
    pieces = []
    for j in range(8):
        even, odd = osc[pl.ds(16 * j, 8), :], osc[pl.ds(16 * j + 8, 8), :]
        if j < 4:
            pieces.append(jnp.where(low, even, pltpu.roll(odd, HD, 1)))
        else:
            pieces.append(jnp.where(low, pltpu.roll(even, HD, 1), odd))
    attended = jnp.concatenate(pieces, axis=1).astype(BF16)
    after = hidden
    for i in range(OCHUNK):
        loads[("wo", i)].wait()
        after = after + jnp.dot(
            attended[:, i * orows : (i + 1) * orows], wo[i * orows : (i + 1) * orows, :],
            preferred_element_type=F32,
        )
    after = after.astype(BF16).astype(F32)
    loads["ffn_gain"].wait()
    expert_in = rms_norm(after, ffn_gain_ref[...].astype(F32).reshape(1, D)).astype(F32)

    for i in range(2):
        half = (c + i) % 2
        cols = pl.ds(pl.multiple_of(half * HALF, HALF), HALF)
        load("wg", wg_hbm.at[0, :, cols], wexp.at[i], esem)
        load("wu", wu_hbm.at[0, :, cols], wexp.at[2 + i], esem)
        load("wd", wd_hbm.at[0, :, cols], wexp.at[4 + i], esem)

    pl.semaphore_wait(barrier, len(partners))
    for i, (k, o) in enumerate(rowdev):
        copy = remote(
            table.at[c], table.at[2 * k + c], tsend, trecv.at[(0, 2, 1, 1)[k]],
            dev(0, 0, 4 - XOFF[k], (c + o) % 2),
        )
        copy.start()

    mine = jnp.where(c == 0, expert_in[:, :HALF], expert_in[:, HALF:])
    xin[c] = mine.astype(BF16)
    xsend[...] = jnp.where(c == 0, expert_in[:, HALF:], expert_in[:, :HALF]).astype(BF16)
    swap = remote(xsend, xin.at[c], xs_sem, xr_sem, dev(0, 0, 0, 1 - c))
    swap.start()
    far = [
        remote(xin.at[c], xfar.at[c], xf_s.at[0], xf_r.at[0], dev(0, 0, 2, c)),
        remote(xsend, xfar.at[c], xf_s.at[1], xf_r.at[1], dev(0, 0, 2, 1 - c)),
    ]
    for copy in far:
        copy.start()

    drain(wkv, kvsem)
    newk_ref[...] = jnp.dot(normed, wkv[0], preferred_element_type=F32).astype(BF16)
    newv_ref[...] = jnp.dot(normed, wkv[1], preferred_element_type=F32).astype(BF16)
    drain(table.at[0], trecv.at[0])

    swap.wait_recv()

    def dispatch(k, tokens_ref, out, ssem, rsem):
        places = jnp.where(table[2 * k : 2 * k + 2].reshape(16, 128) > 0.0, 1.0, 0.0).astype(BF16)
        tokens = tokens_ref[...].astype(F32).reshape(16, HALF).astype(BF16)
        packed = lax.dot_general(
            places, tokens, (((0,), (0,)), ((), ())), preferred_element_type=F32
        ).reshape(16, 8, HALF).astype(BF16)
        out[...] = packed
        blk[k, 0] = packed[0]
        for d in (1, 2, 3, 4, 5, 6, 7, 12, 13, 14, 15, 8, 9, 10, 11):
            remote(
                out.at[d], blk.at[k, d], ssem, rsem.at[d // 4], dev(d // 4, d % 4, 0, c)
            ).start()

    dispatch(0, xin, msg, d1s, d1r)
    def share(k, part):
        remote(blk.at[k, part], pblk.at[k, part], ps, pr.at[k], dev(0, 0, 0, 1 - c)).start()

    def rows(g, start=0):
        return pl.ds(4 * g + start, 4 - start)

    def round_ring(g, part):
        remote(blk.at[0, part], blk.at[2, part], ring_s, ringp_r.at[g], dev(0, 0, 1, c)).start()
        remote(blk.at[0, part], blk.at[3, part], ring_s, ringm_r.at[g], dev(0, 0, 3, c)).start()
        share(0, part)

    round_ring(0, pl.ds(0, 1))
    drain(table.at[pl.ds(0, 2)], trecv.at[2])
    for copy in far:
        copy.wait_recv()
    dispatch(1, xfar, msgfar, d3s, d3r)

    def arrive(k, g, sem):
        start = 4 * g + (1 if g == 0 else 0)
        drain(blk.at[k, pl.ds(start, 4 * g + 4 - start)], sem.at[g])

    for g in GROUPS:
        arrive(0, g, d1r)
        round_ring(g, rows(g, 1 if g == 0 else 0))

    drain(wexp, esem)

    def take(g):
        drain(blk.at[2, rows(g)], ringp_r.at[g])
        share(2, rows(g))
        drain(blk.at[3, rows(g)], ringm_r.at[g])
        share(3, rows(g))

    def take_far(g):
        arrive(1, g, d3r)
        share(1, rows(g))

    spread = (10, 9, 11, 6, 14, 8, 2, 5, 7, 13, 15, 4, 12, 1, 3)
    left, right = pl.ds(0, LEFT), pl.ds(LEFT, RIGHT)

    def experts(k, count, between=()):
        span = pl.ds(k, count)
        own = blk[span].reshape(128 * count, HALF)
        gate, upper = dot_t(wexp[0], own), dot_t(wexp[2], own)
        for j in range(k, k + count):
            drain(pblk.at[j], pr.at[j])
        other = pblk[span].reshape(128 * count, HALF)
        gate, upper = gate + dot_t(wexp[1], other), upper + dot_t(wexp[3], other)
        act = (jax.nn.silu(gate) * upper).T.astype(BF16)
        for g in between:
            take(g)
        for cols, low, high, recv in ((right, LEFT, HALF, orh), (left, 0, LEFT, orr)):
            theirs = jnp.dot(act, wexp[5, :, low:high], preferred_element_type=F32)
            obuf[span, :, :, low:high] = theirs.reshape(count, 16, 8, high - low).astype(BF16)
            for j in range(k, k + count):
                remote(
                    obuf.at[j, :, :, cols], pout.at[j, :, :, cols], os_, recv.at[j], dev(0, 0, 0, 1 - c)
                ).start()
        ofull[span] = jnp.dot(act, wexp[4], preferred_element_type=F32).reshape(count, 16, 8, HALF)

    def send_along(k):
        drain(pout.at[k, :, :, right], orh.at[k])
        total = ofull[k, :, :, LEFT:] + pout[k, :, :, LEFT:].astype(F32)
        if k == 0:
            ghold[...] = total
            return
        rbuf[k, :, :, LEFT:] = total.astype(BF16)
        for h in (2, 3, 1, 0):
            part = pl.ds(4 * h, 4)
            remote(
                rbuf.at[k, part, :, right], gbuf.at[k - 2, part], gs, gr.at[h], dev(0, 0, XOFF[k], c)
            ).start()

    def give_back(k):
        if k == 1:
            drain(pout.at[k, :, :, right], orh.at[k])
        drain(pout.at[k, :, :, left], orr.at[k])
        high = HALF if k == 1 else LEFT
        cols = pl.ds(0, high)
        total = (ofull[k, :, :, :high] + pout[k, :, :, :high].astype(F32)).astype(BF16)
        rbuf[k, :, :, :high] = total
        ybuf[k, 0, :, :high] = total[0]
        for d in spread:
            remote(
                rbuf.at[k, d, :, cols], ybuf.at[k, d, :, cols], ys if k == 1 else yls, yr.at[k],
                dev(4 - d // 4, 4 - d % 4, 0, c),
            ).start()

    def merge(h):
        part = pl.ds(4 * h, 4)
        drain(gbuf.at[:, part], gr.at[h])
        total = ghold[part] + gbuf[0, part].astype(F32) + gbuf[1, part].astype(F32)
        gmsg[part] = total.astype(BF16)
        if h == 0:
            ybuf[0, 0, :, LEFT:] = total[0].astype(BF16)
        for d in spread:
            if d // 4 == h:
                remote(
                    gmsg.at[d], ybuf.at[0, d, :, right], ygs, ygr, dev(4 - d // 4, 4 - d % 4, 0, c)
                ).start()

    take_far(0)
    take_far(1)
    take(0)
    take_far(3)
    take_far(2)
    take(1)
    experts(0, 2)
    take(3)
    take(2)
    give_back(0)
    give_back(1)
    send_along(0)
    experts(2, 2)
    send_along(2)
    send_along(3)
    give_back(2)
    give_back(3)
    merge(3)
    merge(2)
    merge(1)
    merge(0)

    drain(table.at[pl.ds(4, 4)], trecv.at[1])
    def combine(k, low, high):
        scale = table[2 * k : 2 * k + 2].reshape(16, 128).astype(BF16)
        sums = jnp.dot(scale, ybuf[k, :, :, low:high].reshape(128, high - low), preferred_element_type=F32)
        return sums.reshape(2, SEQ, high - low).astype(BF16)

    def deliver(k, o, send, recv, cols):
        core = (c + o) % 2
        remote(
            fsend.at[2 * k + core, :, cols], fbuf.at[k, c, :, cols], send, recv, dev(0, 0, XOFF[k], core)
        ).start()

    for k in (0, 1, 2, 3):
        if k == 1:
            drain(ybuf.at[1, pl.ds(1, 15)], yr.at[1])
            fsend[2:4] = combine(1, 0, HALF)
            deliver(1, 0, fs, fr, pl.ds(0, HALF))
            deliver(1, 1, fs, fr, pl.ds(0, HALF))
            continue
        drain(ybuf.at[k, pl.ds(1, 15), :, left], yr.at[k])
        fsend[2 * k : 2 * k + 2, :, :LEFT] = combine(k, 0, LEFT)
        for o in range(2):
            if k + o > 0:
                deliver(k, o, fls, flr, left)
    drain(ybuf.at[0, pl.ds(1, 15), :, right], ygr)
    fsend[0:2, :, LEFT:] = combine(0, LEFT, HALF)
    deliver(0, 1, fgs, fgr, right)
    fbuf[0, c] = fsend[c]
    drain(fsend.at[pl.ds(0, 5), :, left], flr)
    drain(fsend.at[pl.ds(0, 2)], fr)
    drain(fsend.at[0, :, right], fgr)
    low = fbuf[0, :, :, :LEFT].astype(F32) + fbuf[3, :, :, :LEFT].astype(F32)
    low = low + fbuf[1, :, :, :LEFT].astype(F32) + fbuf[2, :, :, :LEFT].astype(F32)
    high = fbuf[0, :, :, LEFT:].astype(F32) + fbuf[1, :, :, LEFT:].astype(F32)
    total = jnp.concatenate([low, high], axis=-1)
    mixed_ref[:, :HALF] = (after[:, :HALF] + total[0]).astype(BF16)
    mixed_ref[:, HALF:] = (after[:, HALF:] + total[1]).astype(BF16)

    drain(fsend.at[pl.ds(0, 5), :, left], fls)
    drain(fsend.at[pl.ds(0, 2)], fs)
    drain(fsend.at[0, :, right], fgs)
    drain(rbuf.at[pl.ds(2, 2), :, :, right], gs)
    drain(rbuf.at[pl.ds(0, 3), pl.ds(1, 15), :, left], yls)
    drain(gmsg.at[pl.ds(1, 15)], ygs)
    drain(table.at[pl.ds(0, 7)], tsend)
    swap.wait_send()
    for copy in far:
        copy.wait_send()
    drain(msg.at[pl.ds(1, 15)], d1s)
    drain(blk.at[pl.ds(0, 2)], ring_s)
    drain(msgfar.at[pl.ds(1, 15)], d3s)
    drain(blk, ps)
    drain(obuf, os_)
    drain(rbuf.at[1, pl.ds(1, 15)], ys)


def finish(mixed_in, newk_in, newv_in, mixed_ref, newk_ref, newv_ref):
    mixed_ref[...] = mixed_in[...]
    newk_ref[...] = newk_in[...]
    newv_ref[...] = newv_in[...]


def local(*args):
    args = list(args)
    args[11], args[12] = args[11].T, args[12].T
    args[13], args[14] = jnp.swapaxes(args[13], 1, 2), jnp.swapaxes(args[14], 1, 2)
    vmem = pl.BlockSpec(memory_space=pltpu.VMEM)
    smem = pl.BlockSpec(memory_space=pltpu.SMEM)
    hbm = pl.BlockSpec(memory_space=pl.ANY)
    dma = pltpu.SemaphoreType.DMA
    scratch = [
        pltpu.VMEM((SEQ, D), BF16),
        pltpu.VMEM((D,), BF16),
        pltpu.VMEM((D,), BF16),
        pltpu.VMEM((2, SEQ), jnp.int32),
        pltpu.VMEM((2, SEQ), BF16),
        pltpu.VMEM((D, HEADS * HD), BF16),
        pltpu.VMEM((2, D, 128), BF16),
        pltpu.VMEM((SEQ, CACHE, 128), BF16),
        pltpu.VMEM((SEQ, CACHE, 128), BF16),
        pltpu.VMEM((HEADS * HD, D), BF16),
        pltpu.VMEM((6, FFD, HALF), BF16),
        pltpu.VMEM((128, 128), F32),
        pltpu.VMEM((SEQ, HEADS, CACHE), F32),
        pltpu.VMEM((SEQ, 4, HEADS, 512), BF16),
        pltpu.VMEM((512, 384), F32),
        pltpu.VMEM((128, 128), F32),
        pltpu.VMEM((8, SEQ, 128), F32),
        pltpu.VMEM((2, SEQ, HALF), BF16),
        pltpu.VMEM((SEQ, HALF), BF16),
        pltpu.VMEM((2, SEQ, HALF), BF16),
        pltpu.VMEM((16, 8, HALF), BF16),
        pltpu.VMEM((16, 8, HALF), BF16),
        pltpu.VMEM((4, 16, 8, HALF), BF16),
        pltpu.VMEM((4, 16, 8, HALF), BF16),
        pltpu.VMEM((4, 16, 8, HALF), F32),
        pltpu.VMEM((4, 16, 8, HALF), BF16),
        pltpu.VMEM((4, 16, 8, HALF), BF16),
        pltpu.VMEM((4, 16, 8, HALF), BF16),
        pltpu.VMEM((16, 8, RIGHT), F32),
        pltpu.VMEM((2, 16, 8, RIGHT), BF16),
        pltpu.VMEM((16, 8, RIGHT), BF16),
        pltpu.VMEM((4, 16, 8, HALF), BF16),
        pltpu.VMEM((8, SEQ, HALF), BF16),
        pltpu.VMEM((4, 2, SEQ, HALF), BF16),
        dma((QCHUNK + OCHUNK + 7,)), dma, dma,
        dma, dma((3,)),
        dma, dma,
        dma((2,)), dma((2,)),
        dma, dma((4,)),
        dma, dma((4,)),
        dma, dma((4,)), dma((4,)),
        dma, dma((4,)),
        dma, dma((4,)), dma((4,)),
        dma, dma, dma((4,)),
        dma, dma((4,)),
        dma, dma,
        dma, dma, dma, dma, dma, dma,
    ]
    out_shape = (
        jax.ShapeDtypeStruct((SEQ, D), BF16),
        jax.ShapeDtypeStruct((SEQ, 128), BF16),
        jax.ShapeDtypeStruct((SEQ, 128), BF16),
    )
    outs = pl.pallas_call(
        kernel,
        out_shape=tuple(pltpu.VMEM(o.shape, o.dtype) for o in out_shape),
        in_specs=[hbm, smem, hbm, hbm, hbm, hbm, hbm, hbm, smem, hbm, hbm, hbm, hbm, hbm, hbm, hbm],
        out_specs=(vmem, vmem, vmem),
        scratch_shapes=scratch,
        compiler_params=pltpu.CompilerParams(
            collective_id=0, has_side_effects=True, vmem_limit_bytes=60 * 2**20
        ),
        name="layer",
    )(*args)
    return pl.pallas_call(
        finish, out_shape=out_shape, in_specs=[vmem] * 3, out_specs=(vmem,) * 3, name="finish"
    )(*[pltpu.with_memory_space_constraint(o, pltpu.VMEM) for o in outs])


def solution(mesh):
    ep2, ep3 = P("ep", None), P("ep", None, None)
    in_specs = (ep2, P("ep"), ep3, ep3, P(), P(), P(), P(), P(), P(), P(), ep2, ep2, ep3, ep3, ep3)
    return jax.shard_map(
        local, mesh=mesh, in_specs=in_specs, out_specs=(ep2, ep2, ep2), check_vma=False
    )
```

```python
import jax
import jax.numpy as jnp
from jax import lax
from jax.experimental import pallas as pl
from jax.experimental.pallas import tpu as pltpu
from jax.sharding import PartitionSpec as P

D = 2048
HEADS = 16
HD = 64
CACHE = 1024
SEQ = 8
FFD = 352
HALF = D // 2
LEFT = 512
RIGHT = HALF - LEFT
F32 = jnp.float32
BF16 = jnp.bfloat16
MESH = pl.DeviceIdType.MESH
XOFF = (0, 2, 3, 1)
GROUPS = (0, 1, 3, 2)
QCHUNK = 4
OCHUNK = 2


def rms_norm(wide, gain):
    scaled = wide * lax.rsqrt(jnp.mean(wide * wide, axis=-1, keepdims=True) + 1e-06)
    return (scaled * gain).astype(BF16)


def dot_t(a, b):
    return lax.dot_general(a, b, (((1,), (1,)), ((), ())), preferred_element_type=F32)


def kernel(
    hidden_hbm, lengths_hbm, key_hbm, value_hbm, norm_gain_hbm, wq_hbm, wk_hbm, wv_hbm, bias_hbm,
    wo_hbm, ffn_gain_hbm, routing_hbm, route_w_hbm, wg_hbm, wu_hbm, wd_hbm,
    mixed_ref, newk_ref, newv_ref,
    lengths_ref, bias_ref, hidden_ref, norm_gain_ref, ffn_gain_ref, routing_ref, route_w_ref,
    wq, wkv, kc, vc, wo, wexp,
    qs, zs, kp, sums, osc, table, xin, xsend, xfar, msg, msgfar, blk, pblk, ofull, obuf, pout, rbuf, ghold, gbuf, gmsg, ybuf, fsend, fbuf,
    lsem, kvsem, esem, tsend, trecv, xs_sem, xr_sem, xf_s, xf_r, d1s, d1r, d3s, d3r, ring_s, ringp_r, ringm_r,
    ps, pr, os_, orr, orh, ys, yls, yr, gs, gr, ygs, ygr, fs, fr, fls, flr, fgs, fgr,
):
    me = lax.axis_index("ep")
    c = me % 2
    x = (me // 2) % 4
    y = (me // 8) % 4
    z = me // 32

    def dev(dz, dy, dx, core):
        return ((((z + dz) % 4) * 4 + (y + dy) % 4) * 4 + (x + dx) % 4) * 2 + core

    def remote(src, dst, ssem, rsem, target):
        return pltpu.make_async_remote_copy(
            src_ref=src, dst_ref=dst, send_sem=ssem, recv_sem=rsem,
            device_id=(target,), device_id_type=MESH,
        )

    def drain(ref, sem):
        pltpu.make_async_copy(ref, ref, sem).wait()

    loads = {}

    def load(name, src, dst, shared=None):
        copy = pltpu.make_async_copy(src, dst, lsem.at[len(loads)] if shared is None else shared)
        copy.start()
        if shared is None:
            loads[name] = copy

    load("hidden", hidden_hbm, hidden_ref)
    load("norm_gain", norm_gain_hbm, norm_gain_ref)
    load("lengths", lengths_hbm, lengths_ref)
    load("bias", bias_hbm, bias_ref)
    load("routing", routing_hbm, routing_ref)
    load("route_w", route_w_hbm, route_w_ref)
    load("ffn_gain", ffn_gain_hbm, ffn_gain_ref)
    qrows = D // QCHUNK
    for i in range(QCHUNK):
        load(("wq", i), wq_hbm.at[pl.ds(i * qrows, qrows)], wq.at[pl.ds(i * qrows, qrows)])
    load("key", key_hbm, kc)
    load("value", value_hbm, vc)
    orows = HEADS * HD // OCHUNK
    for i in range(OCHUNK):
        load(("wo", i), wo_hbm.at[pl.ds(i * orows, orows)], wo.at[pl.ds(i * orows, orows)])
    load("wk", wk_hbm, wkv.at[0], kvsem)
    load("wv", wv_hbm, wkv.at[1], kvsem)
    barrier = pltpu.get_barrier_semaphore()
    partners = [dev(d // 4, d % 4, 0, c) for d in range(1, 16)]
    row = [(k, core) for k in range(4) for core in range(2)]
    rowdev = [(k, o) for k in range(4) for o in range(2) if k + o > 0]
    partners += [dev(0, 0, 4 - XOFF[k], (c + o) % 2) for k, o in rowdev]
    for target in partners:
        pl.semaphore_signal(barrier, inc=1, device_id=(target,), device_id_type=MESH)

    loads["hidden"].wait()
    loads["norm_gain"].wait()
    hidden = hidden_ref[...].astype(F32)
    normed = rms_norm(hidden, norm_gain_ref[...].astype(F32).reshape(1, D))
    query = jnp.zeros((SEQ, HEADS * HD), F32)
    for i in range(QCHUNK):
        loads[("wq", i)].wait()
        query = query + jnp.dot(
            normed[:, i * qrows : (i + 1) * qrows], wq[i * qrows : (i + 1) * qrows, :],
            preferred_element_type=F32,
        )
    query = query.astype(BF16).astype(F32)
    low = lax.broadcasted_iota(jnp.int32, (SEQ, 128), 1) < HD
    for j in range(8):
        tile = query[:, j * 128 : (j + 1) * 128]
        swapped = pltpu.roll(tile, HD, 1)
        if j < 4:
            even, odd = jnp.where(low, tile, 0.0), jnp.where(low, swapped, 0.0)
        else:
            even, odd = jnp.where(low, 0.0, swapped), jnp.where(low, 0.0, tile)
        qs[pl.ds(16 * j, 8), :] = even
        qs[pl.ds(16 * j + 8, 8), :] = odd

    lane = lax.broadcasted_iota(jnp.int32, (SEQ, 128), 1)
    plane = lane // 8
    lz = (z + plane // 4) % 4
    ly = (y + plane % 4) % 4
    lexpert = 2 * lz + ly // 2
    diagonal = lax.broadcasted_iota(jnp.int32, (SEQ, SEQ), 0) == lax.broadcasted_iota(jnp.int32, (SEQ, SEQ), 1)

    def column(row):
        return jnp.sum(jnp.where(diagonal, row, 0.0), axis=1, keepdims=True)

    loads["routing"].wait()
    loads["route_w"].wait()
    routing = routing_ref[...].astype(F32)
    route_w = route_w_ref[...].astype(F32)
    lexpert = lexpert.astype(F32)
    is_first = jnp.abs(lexpert - column(routing[0:1])) < 0.5
    is_second = jnp.abs(lexpert - column(routing[1:2])) < 0.5
    named = jnp.where(is_first | is_second, 1.0, 0.0).astype(F32)
    tri = (
        lax.broadcasted_iota(jnp.int32, (SEQ, SEQ), 0) >= lax.broadcasted_iota(jnp.int32, (SEQ, SEQ), 1)
    ).astype(F32)
    rank = jnp.dot(tri, named, preferred_element_type=F32)
    here = (jnp.abs(rank - 1.0 - (lane % 4).astype(F32)) < 0.5) & ((lane // 4) % 2 == c)
    weight = jnp.where(is_first, column(route_w[0:1]), jnp.where(is_second, column(route_w[1:2]), 0.0))
    table[c] = jnp.where(here, weight, 0.0)

    loads["key"].wait()
    loads["lengths"].wait()
    loads["bias"].wait()
    sub = lax.broadcasted_iota(jnp.int32, (HEADS, 128), 0)
    bias = jnp.zeros((HEADS, 128), F32)
    for h in range(HEADS):
        bias = jnp.where(sub == h, bias_ref[h], bias)
    bias = jnp.concatenate([bias] * 8, axis=1)
    position = lax.broadcasted_iota(jnp.int32, (HEADS, CACHE), 1)
    for s in range(SEQ):
        q = qs[pl.ds(s, HEADS, stride=SEQ), :].astype(BF16)
        scores = lax.dot_general(
            q, kc[s], (((1,), (1,)), ((), ())), preferred_element_type=F32
        ) * (HD ** -0.5) + bias
        soft = jnp.log(1.0 + jnp.exp(-jnp.abs(scores)))
        used = position < lengths_ref[s]
        keep = jnp.where(used, -(jnp.maximum(scores, 0.0) + soft), 0.0)
        zs[s] = jnp.where(used, jnp.minimum(scores, 0.0) - soft, -1e30)
        high = keep.astype(BF16)
        rest = (keep - high.astype(F32)).astype(BF16)
        for b in range(4):
            kp[s, b, :, :256] = high[:, b * 256 : (b + 1) * 256]
            kp[s, b, :, 256:] = rest[:, b * 256 : (b + 1) * 256]
    col = lax.broadcasted_iota(jnp.int32, (512, 384), 1)
    below = (lax.broadcasted_iota(jnp.int32, (512, 384), 0) % 256 > col) | (col >= 256)
    below = jnp.where(below, 1.0, 0.0).astype(BF16)
    sums[...] = jnp.dot(kp[...].reshape(512, 512), below, preferred_element_type=F32)
    loads["value"].wait()
    for s in range(SEQ):
        carry = jnp.zeros((HEADS, 128), F32)
        parts = [None] * 4
        for b in (3, 2, 1, 0):
            piece = sums[pl.ds(s * 64 + b * 16, 16), :]
            after = piece[:, :256] + jnp.concatenate([carry, carry], axis=1)
            parts[b] = jnp.exp(zs[s, :, b * 256 : (b + 1) * 256] + after).astype(BF16)
            carry = carry + piece[:, 256:]
        weights = jnp.concatenate(parts, axis=1)
        out = jnp.dot(weights, vc[s], preferred_element_type=F32)
        osc[pl.ds(s, HEADS, stride=SEQ), :] = out
    pieces = []
    for j in range(8):
        even, odd = osc[pl.ds(16 * j, 8), :], osc[pl.ds(16 * j + 8, 8), :]
        if j < 4:
            pieces.append(jnp.where(low, even, pltpu.roll(odd, HD, 1)))
        else:
            pieces.append(jnp.where(low, pltpu.roll(even, HD, 1), odd))
    attended = jnp.concatenate(pieces, axis=1).astype(BF16)
    after = hidden
    for i in range(OCHUNK):
        loads[("wo", i)].wait()
        after = after + jnp.dot(
            attended[:, i * orows : (i + 1) * orows], wo[i * orows : (i + 1) * orows, :],
            preferred_element_type=F32,
        )
    after = after.astype(BF16).astype(F32)
    loads["ffn_gain"].wait()
    expert_in = rms_norm(after, ffn_gain_ref[...].astype(F32).reshape(1, D)).astype(F32)

    for i in range(2):
        half = (c + i) % 2
        cols = pl.ds(pl.multiple_of(half * HALF, HALF), HALF)
        load("wg", wg_hbm.at[0, :, cols], wexp.at[i], esem)
        load("wu", wu_hbm.at[0, :, cols], wexp.at[2 + i], esem)
        load("wd", wd_hbm.at[0, :, cols], wexp.at[4 + i], esem)

    pl.semaphore_wait(barrier, len(partners))
    for i, (k, o) in enumerate(rowdev):
        copy = remote(
            table.at[c], table.at[2 * k + c], tsend, trecv.at[(0, 2, 1, 1)[k]],
            dev(0, 0, 4 - XOFF[k], (c + o) % 2),
        )
        copy.start()

    mine = jnp.where(c == 0, expert_in[:, :HALF], expert_in[:, HALF:])
    xin[c] = mine.astype(BF16)
    xsend[...] = jnp.where(c == 0, expert_in[:, HALF:], expert_in[:, :HALF]).astype(BF16)
    swap = remote(xsend, xin.at[c], xs_sem, xr_sem, dev(0, 0, 0, 1 - c))
    swap.start()
    far = [
        remote(xin.at[c], xfar.at[c], xf_s.at[0], xf_r.at[0], dev(0, 0, 2, c)),
        remote(xsend, xfar.at[c], xf_s.at[1], xf_r.at[1], dev(0, 0, 2, 1 - c)),
    ]
    for copy in far:
        copy.start()

    drain(wkv, kvsem)
    newk_ref[...] = jnp.dot(normed, wkv[0], preferred_element_type=F32).astype(BF16)
    newv_ref[...] = jnp.dot(normed, wkv[1], preferred_element_type=F32).astype(BF16)
    drain(table.at[0], trecv.at[0])

    swap.wait_recv()

    def dispatch(k, tokens_ref, out, ssem, rsem):
        places = jnp.where(table[2 * k : 2 * k + 2].reshape(16, 128) > 0.0, 1.0, 0.0).astype(BF16)
        tokens = tokens_ref[...].astype(F32).reshape(16, HALF).astype(BF16)
        packed = lax.dot_general(
            places, tokens, (((0,), (0,)), ((), ())), preferred_element_type=F32
        ).reshape(16, 8, HALF).astype(BF16)
        out[...] = packed
        blk[k, 0] = packed[0]
        for d in (1, 2, 3, 4, 5, 6, 7, 12, 13, 14, 15, 8, 9, 10, 11):
            remote(
                out.at[d], blk.at[k, d], ssem, rsem.at[d // 4], dev(d // 4, d % 4, 0, c)
            ).start()

    dispatch(0, xin, msg, d1s, d1r)
    def share(k, part):
        remote(blk.at[k, part], pblk.at[k, part], ps, pr.at[k], dev(0, 0, 0, 1 - c)).start()

    def rows(g, start=0):
        return pl.ds(4 * g + start, 4 - start)

    def round_ring(g, part):
        remote(blk.at[0, part], blk.at[2, part], ring_s, ringp_r.at[g], dev(0, 0, 1, c)).start()
        remote(blk.at[0, part], blk.at[3, part], ring_s, ringm_r.at[g], dev(0, 0, 3, c)).start()
        share(0, part)

    round_ring(0, pl.ds(0, 1))
    drain(table.at[pl.ds(0, 2)], trecv.at[2])
    for copy in far:
        copy.wait_recv()
    dispatch(1, xfar, msgfar, d3s, d3r)

    def arrive(k, g, sem):
        start = 4 * g + (1 if g == 0 else 0)
        drain(blk.at[k, pl.ds(start, 4 * g + 4 - start)], sem.at[g])

    for g in GROUPS:
        arrive(0, g, d1r)
        round_ring(g, rows(g, 1 if g == 0 else 0))

    drain(wexp, esem)

    def take(g):
        drain(blk.at[2, rows(g)], ringp_r.at[g])
        share(2, rows(g))
        drain(blk.at[3, rows(g)], ringm_r.at[g])
        share(3, rows(g))

    def take_far(g):
        arrive(1, g, d3r)
        share(1, rows(g))

    spread = (10, 9, 11, 6, 14, 8, 2, 5, 7, 13, 15, 4, 12, 1, 3)
    left, right = pl.ds(0, LEFT), pl.ds(LEFT, RIGHT)

    def experts(k, count, between=()):
        span = pl.ds(k, count)
        own = blk[span].reshape(128 * count, HALF)
        gate, upper = dot_t(wexp[0], own), dot_t(wexp[2], own)
        for j in range(k, k + count):
            drain(pblk.at[j], pr.at[j])
        other = pblk[span].reshape(128 * count, HALF)
        gate, upper = gate + dot_t(wexp[1], other), upper + dot_t(wexp[3], other)
        act = (jax.nn.silu(gate) * upper).T.astype(BF16)
        for step, g in between:
            step(g)
        for cols, low, high, recv in ((right, LEFT, HALF, orh), (left, 0, LEFT, orr)):
            theirs = jnp.dot(act, wexp[5, :, low:high], preferred_element_type=F32)
            obuf[span, :, :, low:high] = theirs.reshape(count, 16, 8, high - low).astype(BF16)
            for j in range(k, k + count):
                remote(
                    obuf.at[j, :, :, cols], pout.at[j, :, :, cols], os_, recv.at[j], dev(0, 0, 0, 1 - c)
                ).start()
        ofull[span] = jnp.dot(act, wexp[4], preferred_element_type=F32).reshape(count, 16, 8, HALF)

    def send_along(k):
        drain(pout.at[k, :, :, right], orh.at[k])
        total = ofull[k, :, :, LEFT:] + pout[k, :, :, LEFT:].astype(F32)
        if k == 0:
            ghold[...] = total
            return
        rbuf[k, :, :, LEFT:] = total.astype(BF16)
        for h in (2, 3, 1, 0):
            part = pl.ds(4 * h, 4)
            remote(
                rbuf.at[k, part, :, right], gbuf.at[k - 2, part], gs, gr.at[h], dev(0, 0, XOFF[k], c)
            ).start()

    def give_back(k):
        if k == 1:
            drain(pout.at[k, :, :, right], orh.at[k])
        drain(pout.at[k, :, :, left], orr.at[k])
        high = HALF if k == 1 else LEFT
        cols = pl.ds(0, high)
        total = (ofull[k, :, :, :high] + pout[k, :, :, :high].astype(F32)).astype(BF16)
        rbuf[k, :, :, :high] = total
        ybuf[k, 0, :, :high] = total[0]
        for d in spread:
            remote(
                rbuf.at[k, d, :, cols], ybuf.at[k, d, :, cols], ys if k == 1 else yls, yr.at[k],
                dev(4 - d // 4, 4 - d % 4, 0, c),
            ).start()

    def merge(h):
        part = pl.ds(4 * h, 4)
        drain(gbuf.at[:, part], gr.at[h])
        total = ghold[part] + gbuf[0, part].astype(F32) + gbuf[1, part].astype(F32)
        gmsg[part] = total.astype(BF16)
        if h == 0:
            ybuf[0, 0, :, LEFT:] = total[0].astype(BF16)
        for d in spread:
            if d // 4 == h:
                remote(
                    gmsg.at[d], ybuf.at[0, d, :, right], ygs, ygr, dev(4 - d // 4, 4 - d % 4, 0, c)
                ).start()

    take_far(0)
    experts(0, 1, ((take_far, 1),))
    take(0)
    take_far(3)
    take_far(2)
    take(1)
    give_back(0)
    send_along(0)
    experts(1, 1)
    take(3)
    take(2)
    give_back(1)
    experts(2, 2)
    send_along(2)
    send_along(3)
    give_back(2)
    give_back(3)
    merge(3)
    merge(2)
    merge(1)
    merge(0)

    drain(table.at[pl.ds(4, 4)], trecv.at[1])
    def combine(k, low, high):
        scale = table[2 * k : 2 * k + 2].reshape(16, 128).astype(BF16)
        sums = jnp.dot(scale, ybuf[k, :, :, low:high].reshape(128, high - low), preferred_element_type=F32)
        return sums.reshape(2, SEQ, high - low).astype(BF16)

    def deliver(k, o, send, recv, cols):
        core = (c + o) % 2
        remote(
            fsend.at[2 * k + core, :, cols], fbuf.at[k, c, :, cols], send, recv, dev(0, 0, XOFF[k], core)
        ).start()

    for k in (0, 1, 2, 3):
        if k == 1:
            drain(ybuf.at[1, pl.ds(1, 15)], yr.at[1])
            fsend[2:4] = combine(1, 0, HALF)
            deliver(1, 0, fs, fr, pl.ds(0, HALF))
            deliver(1, 1, fs, fr, pl.ds(0, HALF))
            continue
        drain(ybuf.at[k, pl.ds(1, 15), :, left], yr.at[k])
        fsend[2 * k : 2 * k + 2, :, :LEFT] = combine(k, 0, LEFT)
        for o in range(2):
            if k + o > 0:
                deliver(k, o, fls, flr, left)
    drain(ybuf.at[0, pl.ds(1, 15), :, right], ygr)
    fsend[0:2, :, LEFT:] = combine(0, LEFT, HALF)
    deliver(0, 1, fgs, fgr, right)
    fbuf[0, c] = fsend[c]
    drain(fsend.at[pl.ds(0, 5), :, left], flr)
    drain(fsend.at[pl.ds(0, 2)], fr)
    drain(fsend.at[0, :, right], fgr)
    low = fbuf[0, :, :, :LEFT].astype(F32) + fbuf[3, :, :, :LEFT].astype(F32)
    low = low + fbuf[1, :, :, :LEFT].astype(F32) + fbuf[2, :, :, :LEFT].astype(F32)
    high = fbuf[0, :, :, LEFT:].astype(F32) + fbuf[1, :, :, LEFT:].astype(F32)
    total = jnp.concatenate([low, high], axis=-1)
    mixed_ref[:, :HALF] = (after[:, :HALF] + total[0]).astype(BF16)
    mixed_ref[:, HALF:] = (after[:, HALF:] + total[1]).astype(BF16)

    drain(fsend.at[pl.ds(0, 5), :, left], fls)
    drain(fsend.at[pl.ds(0, 2)], fs)
    drain(fsend.at[0, :, right], fgs)
    drain(rbuf.at[pl.ds(2, 2), :, :, right], gs)
    drain(rbuf.at[pl.ds(0, 3), pl.ds(1, 15), :, left], yls)
    drain(gmsg.at[pl.ds(1, 15)], ygs)
    drain(table.at[pl.ds(0, 7)], tsend)
    swap.wait_send()
    for copy in far:
        copy.wait_send()
    drain(msg.at[pl.ds(1, 15)], d1s)
    drain(blk.at[pl.ds(0, 2)], ring_s)
    drain(msgfar.at[pl.ds(1, 15)], d3s)
    drain(blk, ps)
    drain(obuf, os_)
    drain(rbuf.at[1, pl.ds(1, 15)], ys)


def finish(mixed_in, newk_in, newv_in, mixed_ref, newk_ref, newv_ref):
    mixed_ref[...] = mixed_in[...]
    newk_ref[...] = newk_in[...]
    newv_ref[...] = newv_in[...]


def local(*args):
    args = list(args)
    args[11], args[12] = args[11].T, args[12].T
    args[13], args[14] = jnp.swapaxes(args[13], 1, 2), jnp.swapaxes(args[14], 1, 2)
    vmem = pl.BlockSpec(memory_space=pltpu.VMEM)
    hbm = pl.BlockSpec(memory_space=pl.ANY)
    dma = pltpu.SemaphoreType.DMA
    scratch = [
        pltpu.SMEM((SEQ,), jnp.int32),
        pltpu.SMEM((HEADS,), F32),
        pltpu.VMEM((SEQ, D), BF16),
        pltpu.VMEM((D,), BF16),
        pltpu.VMEM((D,), BF16),
        pltpu.VMEM((2, SEQ), jnp.int32),
        pltpu.VMEM((2, SEQ), BF16),
        pltpu.VMEM((D, HEADS * HD), BF16),
        pltpu.VMEM((2, D, 128), BF16),
        pltpu.VMEM((SEQ, CACHE, 128), BF16),
        pltpu.VMEM((SEQ, CACHE, 128), BF16),
        pltpu.VMEM((HEADS * HD, D), BF16),
        pltpu.VMEM((6, FFD, HALF), BF16),
        pltpu.VMEM((128, 128), F32),
        pltpu.VMEM((SEQ, HEADS, CACHE), F32),
        pltpu.VMEM((SEQ, 4, HEADS, 512), BF16),
        pltpu.VMEM((512, 384), F32),
        pltpu.VMEM((128, 128), F32),
        pltpu.VMEM((8, SEQ, 128), F32),
        pltpu.VMEM((2, SEQ, HALF), BF16),
        pltpu.VMEM((SEQ, HALF), BF16),
        pltpu.VMEM((2, SEQ, HALF), BF16),
        pltpu.VMEM((16, 8, HALF), BF16),
        pltpu.VMEM((16, 8, HALF), BF16),
        pltpu.VMEM((4, 16, 8, HALF), BF16),
        pltpu.VMEM((4, 16, 8, HALF), BF16),
        pltpu.VMEM((4, 16, 8, HALF), F32),
        pltpu.VMEM((4, 16, 8, HALF), BF16),
        pltpu.VMEM((4, 16, 8, HALF), BF16),
        pltpu.VMEM((4, 16, 8, HALF), BF16),
        pltpu.VMEM((16, 8, RIGHT), F32),
        pltpu.VMEM((2, 16, 8, RIGHT), BF16),
        pltpu.VMEM((16, 8, RIGHT), BF16),
        pltpu.VMEM((4, 16, 8, HALF), BF16),
        pltpu.VMEM((8, SEQ, HALF), BF16),
        pltpu.VMEM((4, 2, SEQ, HALF), BF16),
        dma((QCHUNK + OCHUNK + 9,)), dma, dma,
        dma, dma((3,)),
        dma, dma,
        dma((2,)), dma((2,)),
        dma, dma((4,)),
        dma, dma((4,)),
        dma, dma((4,)), dma((4,)),
        dma, dma((4,)),
        dma, dma((4,)), dma((4,)),
        dma, dma, dma((4,)),
        dma, dma((4,)),
        dma, dma,
        dma, dma, dma, dma, dma, dma,
    ]
    out_shape = (
        jax.ShapeDtypeStruct((SEQ, D), BF16),
        jax.ShapeDtypeStruct((SEQ, 128), BF16),
        jax.ShapeDtypeStruct((SEQ, 128), BF16),
    )
    outs = pl.pallas_call(
        kernel,
        out_shape=tuple(pltpu.VMEM(o.shape, o.dtype) for o in out_shape),
        in_specs=[hbm] * 16,
        out_specs=(vmem, vmem, vmem),
        scratch_shapes=scratch,
        compiler_params=pltpu.CompilerParams(
            collective_id=0, has_side_effects=True, vmem_limit_bytes=60 * 2**20
        ),
        name="layer",
    )(*args)
    return pl.pallas_call(
        finish, out_shape=out_shape, in_specs=[vmem] * 3, out_specs=(vmem,) * 3, name="finish"
    )(*[pltpu.with_memory_space_constraint(o, pltpu.VMEM) for o in outs])


def solution(mesh):
    ep2, ep3 = P("ep", None), P("ep", None, None)
    in_specs = (ep2, P("ep"), ep3, ep3, P(), P(), P(), P(), P(), P(), P(), ep2, ep2, ep3, ep3, ep3)
    return jax.shard_map(
        local, mesh=mesh, in_specs=in_specs, out_specs=(ep2, ep2, ep2), check_vma=False
    )
```

```python
import jax
import jax.numpy as jnp
from jax import lax
from jax.experimental import pallas as pl
from jax.experimental.pallas import tpu as pltpu
from jax.sharding import PartitionSpec as P

D = 2048
HEADS = 16
HD = 64
CACHE = 1024
SEQ = 8
FFD = 352
HALF = D // 2
LEFT = 640
RIGHT = HALF - LEFT
F32 = jnp.float32
BF16 = jnp.bfloat16
MESH = pl.DeviceIdType.MESH
XOFF = (0, 2, 3, 1)
GROUPS = (0, 1, 3, 2)
QCHUNK = 4
OCHUNK = 2


def rms_norm(wide, gain):
    scaled = wide * lax.rsqrt(jnp.mean(wide * wide, axis=-1, keepdims=True) + 1e-06)
    return (scaled * gain).astype(BF16)


def dot_t(a, b):
    return lax.dot_general(a, b, (((1,), (1,)), ((), ())), preferred_element_type=F32)


def kernel(
    hidden_hbm, lengths_hbm, key_hbm, value_hbm, norm_gain_hbm, wq_hbm, wk_hbm, wv_hbm, bias_hbm,
    wo_hbm, ffn_gain_hbm, routing_hbm, route_w_hbm, wg_hbm, wu_hbm, wd_hbm,
    mixed_ref, newk_ref, newv_ref,
    lengths_ref, bias_ref, hidden_ref, norm_gain_ref, ffn_gain_ref, routing_ref, route_w_ref,
    wq, wkv, kc, vc, wo, wexp,
    qs, zs, kp, sums, osc, table, xin, xsend, xfar, msg, msgfar, blk, pblk, ofull, obuf, pout, rbuf, ghold, gbuf, gmsg, ybuf, fsend, fbuf,
    lsem, kvsem, esem, tsend, trecv, xs_sem, xr_sem, xf_s, xf_r, d1s, d1r, d3s, d3r, ring_s, ringp_r, ringm_r,
    ps, pr, os_, orr, orh, ys, yls, yr, gs, gr, ygs, ygr, fs, fr, fls, flr, fgs, fgr,
):
    me = lax.axis_index("ep")
    c = me % 2
    x = (me // 2) % 4
    y = (me // 8) % 4
    z = me // 32

    def dev(dz, dy, dx, core):
        return ((((z + dz) % 4) * 4 + (y + dy) % 4) * 4 + (x + dx) % 4) * 2 + core

    def remote(src, dst, ssem, rsem, target):
        return pltpu.make_async_remote_copy(
            src_ref=src, dst_ref=dst, send_sem=ssem, recv_sem=rsem,
            device_id=(target,), device_id_type=MESH,
        )

    def drain(ref, sem):
        pltpu.make_async_copy(ref, ref, sem).wait()

    loads = {}

    def load(name, src, dst, shared=None):
        copy = pltpu.make_async_copy(src, dst, lsem.at[len(loads)] if shared is None else shared)
        copy.start()
        if shared is None:
            loads[name] = copy

    load("hidden", hidden_hbm, hidden_ref)
    load("norm_gain", norm_gain_hbm, norm_gain_ref)
    load("lengths", lengths_hbm, lengths_ref)
    load("bias", bias_hbm, bias_ref)
    load("routing", routing_hbm, routing_ref)
    load("route_w", route_w_hbm, route_w_ref)
    load("ffn_gain", ffn_gain_hbm, ffn_gain_ref)
    qrows = D // QCHUNK
    for i in range(QCHUNK):
        load(("wq", i), wq_hbm.at[pl.ds(i * qrows, qrows)], wq.at[pl.ds(i * qrows, qrows)])
    load("key", key_hbm, kc)
    load("value", value_hbm, vc)
    orows = HEADS * HD // OCHUNK
    for i in range(OCHUNK):
        load(("wo", i), wo_hbm.at[pl.ds(i * orows, orows)], wo.at[pl.ds(i * orows, orows)])
    load("wk", wk_hbm, wkv.at[0], kvsem)
    load("wv", wv_hbm, wkv.at[1], kvsem)
    barrier = pltpu.get_barrier_semaphore()
    partners = [dev(d // 4, d % 4, 0, c) for d in range(1, 16)]
    row = [(k, core) for k in range(4) for core in range(2)]
    rowdev = [(k, o) for k in range(4) for o in range(2) if k + o > 0]
    partners += [dev(0, 0, 4 - XOFF[k], (c + o) % 2) for k, o in rowdev]
    for target in partners:
        pl.semaphore_signal(barrier, inc=1, device_id=(target,), device_id_type=MESH)

    loads["hidden"].wait()
    loads["norm_gain"].wait()
    hidden = hidden_ref[...].astype(F32)
    normed = rms_norm(hidden, norm_gain_ref[...].astype(F32).reshape(1, D))
    lane = lax.broadcasted_iota(jnp.int32, (SEQ, 128), 1)
    plane = lane // 8
    lz = (z + plane // 4) % 4
    ly = (y + plane % 4) % 4
    lexpert = 2 * lz + ly // 2
    diagonal = lax.broadcasted_iota(jnp.int32, (SEQ, SEQ), 0) == lax.broadcasted_iota(jnp.int32, (SEQ, SEQ), 1)

    def column(row):
        return jnp.sum(jnp.where(diagonal, row, 0.0), axis=1, keepdims=True)

    loads["routing"].wait()
    loads["route_w"].wait()
    routing = routing_ref[...].astype(F32)
    route_w = route_w_ref[...].astype(F32)
    lexpert = lexpert.astype(F32)
    is_first = jnp.abs(lexpert - column(routing[0:1])) < 0.5
    is_second = jnp.abs(lexpert - column(routing[1:2])) < 0.5
    named = jnp.where(is_first | is_second, 1.0, 0.0).astype(F32)
    tri = (
        lax.broadcasted_iota(jnp.int32, (SEQ, SEQ), 0) >= lax.broadcasted_iota(jnp.int32, (SEQ, SEQ), 1)
    ).astype(F32)
    rank = jnp.dot(tri, named, preferred_element_type=F32)
    here = (jnp.abs(rank - 1.0 - (lane % 4).astype(F32)) < 0.5) & ((lane // 4) % 2 == c)
    weight = jnp.where(is_first, column(route_w[0:1]), jnp.where(is_second, column(route_w[1:2]), 0.0))
    table[c] = jnp.where(here, weight, 0.0)

    query = jnp.zeros((SEQ, HEADS * HD), F32)
    for i in range(QCHUNK):
        loads[("wq", i)].wait()
        query = query + jnp.dot(
            normed[:, i * qrows : (i + 1) * qrows], wq[i * qrows : (i + 1) * qrows, :],
            preferred_element_type=F32,
        )
    query = query.astype(BF16).astype(F32)
    low = lax.broadcasted_iota(jnp.int32, (SEQ, 128), 1) < HD
    for j in range(8):
        tile = query[:, j * 128 : (j + 1) * 128]
        swapped = pltpu.roll(tile, HD, 1)
        if j < 4:
            even, odd = jnp.where(low, tile, 0.0), jnp.where(low, swapped, 0.0)
        else:
            even, odd = jnp.where(low, 0.0, swapped), jnp.where(low, 0.0, tile)
        qs[pl.ds(16 * j, 8), :] = even
        qs[pl.ds(16 * j + 8, 8), :] = odd

    loads["key"].wait()
    loads["lengths"].wait()
    loads["bias"].wait()
    sub = lax.broadcasted_iota(jnp.int32, (HEADS, 128), 0)
    bias = jnp.zeros((HEADS, 128), F32)
    for h in range(HEADS):
        bias = jnp.where(sub == h, bias_ref[h], bias)
    bias = jnp.concatenate([bias] * 8, axis=1)
    position = lax.broadcasted_iota(jnp.int32, (HEADS, CACHE), 1)
    for s in range(SEQ):
        q = qs[pl.ds(s, HEADS, stride=SEQ), :].astype(BF16)
        scores = lax.dot_general(
            q, kc[s], (((1,), (1,)), ((), ())), preferred_element_type=F32
        ) * (HD ** -0.5) + bias
        soft = jnp.log(1.0 + jnp.exp(-jnp.abs(scores)))
        used = position < lengths_ref[s]
        keep = jnp.where(used, -(jnp.maximum(scores, 0.0) + soft), 0.0)
        zs[s] = jnp.where(used, jnp.minimum(scores, 0.0) - soft, -1e30)
        high = keep.astype(BF16)
        rest = (keep - high.astype(F32)).astype(BF16)
        for b in range(4):
            kp[s, b, :, :256] = high[:, b * 256 : (b + 1) * 256]
            kp[s, b, :, 256:] = rest[:, b * 256 : (b + 1) * 256]
    col = lax.broadcasted_iota(jnp.int32, (512, 384), 1)
    below = (lax.broadcasted_iota(jnp.int32, (512, 384), 0) % 256 > col) | (col >= 256)
    below = jnp.where(below, 1.0, 0.0).astype(BF16)
    sums[...] = jnp.dot(kp[...].reshape(512, 512), below, preferred_element_type=F32)
    loads["value"].wait()
    for s in range(SEQ):
        carry = jnp.zeros((HEADS, 128), F32)
        parts = [None] * 4
        for b in (3, 2, 1, 0):
            piece = sums[pl.ds(s * 64 + b * 16, 16), :]
            after = piece[:, :256] + jnp.concatenate([carry, carry], axis=1)
            parts[b] = jnp.exp(zs[s, :, b * 256 : (b + 1) * 256] + after).astype(BF16)
            carry = carry + piece[:, 256:]
        weights = jnp.concatenate(parts, axis=1)
        out = jnp.dot(weights, vc[s], preferred_element_type=F32)
        osc[pl.ds(s, HEADS, stride=SEQ), :] = out
    pieces = []
    for j in range(8):
        even, odd = osc[pl.ds(16 * j, 8), :], osc[pl.ds(16 * j + 8, 8), :]
        if j < 4:
            pieces.append(jnp.where(low, even, pltpu.roll(odd, HD, 1)))
        else:
            pieces.append(jnp.where(low, pltpu.roll(even, HD, 1), odd))
    attended = jnp.concatenate(pieces, axis=1).astype(BF16)
    after = hidden
    for i in range(OCHUNK):
        loads[("wo", i)].wait()
        after = after + jnp.dot(
            attended[:, i * orows : (i + 1) * orows], wo[i * orows : (i + 1) * orows, :],
            preferred_element_type=F32,
        )
    after = after.astype(BF16).astype(F32)
    loads["ffn_gain"].wait()
    expert_in = rms_norm(after, ffn_gain_ref[...].astype(F32).reshape(1, D)).astype(F32)

    for i in range(2):
        half = (c + i) % 2
        cols = pl.ds(pl.multiple_of(half * HALF, HALF), HALF)
        load("wg", wg_hbm.at[0, :, cols], wexp.at[i], esem)
        load("wu", wu_hbm.at[0, :, cols], wexp.at[2 + i], esem)
        load("wd", wd_hbm.at[0, :, cols], wexp.at[4 + i], esem)

    pl.semaphore_wait(barrier, len(partners))
    for i, (k, o) in enumerate(rowdev):
        copy = remote(
            table.at[c], table.at[2 * k + c], tsend, trecv.at[(0, 2, 1, 1)[k]],
            dev(0, 0, 4 - XOFF[k], (c + o) % 2),
        )
        copy.start()

    mine = jnp.where(c == 0, expert_in[:, :HALF], expert_in[:, HALF:])
    xin[c] = mine.astype(BF16)
    xsend[...] = jnp.where(c == 0, expert_in[:, HALF:], expert_in[:, :HALF]).astype(BF16)
    swap = remote(xsend, xin.at[c], xs_sem, xr_sem, dev(0, 0, 0, 1 - c))
    swap.start()
    far = [
        remote(xin.at[c], xfar.at[c], xf_s.at[0], xf_r.at[0], dev(0, 0, 2, c)),
        remote(xsend, xfar.at[c], xf_s.at[1], xf_r.at[1], dev(0, 0, 2, 1 - c)),
    ]
    for copy in far:
        copy.start()

    drain(wkv, kvsem)
    newk_ref[...] = jnp.dot(normed, wkv[0], preferred_element_type=F32).astype(BF16)
    newv_ref[...] = jnp.dot(normed, wkv[1], preferred_element_type=F32).astype(BF16)
    drain(table.at[0], trecv.at[0])

    swap.wait_recv()

    def dispatch(k, tokens_ref, out, ssem, rsem):
        places = jnp.where(table[2 * k : 2 * k + 2].reshape(16, 128) > 0.0, 1.0, 0.0).astype(BF16)
        tokens = tokens_ref[...].astype(F32).reshape(16, HALF).astype(BF16)
        packed = lax.dot_general(
            places, tokens, (((0,), (0,)), ((), ())), preferred_element_type=F32
        ).reshape(16, 8, HALF).astype(BF16)
        out[...] = packed
        blk[k, 0] = packed[0]
        for d in (1, 2, 3, 4, 5, 6, 7, 12, 13, 14, 15, 8, 9, 10, 11):
            remote(
                out.at[d], blk.at[k, d], ssem, rsem.at[d // 4], dev(d // 4, d % 4, 0, c)
            ).start()

    dispatch(0, xin, msg, d1s, d1r)
    def share(k, part):
        remote(blk.at[k, part], pblk.at[k, part], ps, pr.at[k], dev(0, 0, 0, 1 - c)).start()

    def rows(g, start=0):
        return pl.ds(4 * g + start, 4 - start)

    def round_ring(g, part):
        remote(blk.at[0, part], blk.at[2, part], ring_s, ringp_r.at[g], dev(0, 0, 1, c)).start()
        remote(blk.at[0, part], blk.at[3, part], ring_s, ringm_r.at[g], dev(0, 0, 3, c)).start()
        share(0, part)

    round_ring(0, pl.ds(0, 1))
    drain(table.at[pl.ds(0, 2)], trecv.at[2])
    for copy in far:
        copy.wait_recv()
    dispatch(1, xfar, msgfar, d3s, d3r)

    def arrive(k, g, sem):
        start = 4 * g + (1 if g == 0 else 0)
        drain(blk.at[k, pl.ds(start, 4 * g + 4 - start)], sem.at[g])

    for g in GROUPS:
        arrive(0, g, d1r)
        round_ring(g, rows(g, 1 if g == 0 else 0))

    drain(wexp, esem)

    def take(g):
        drain(blk.at[2, rows(g)], ringp_r.at[g])
        share(2, rows(g))
        drain(blk.at[3, rows(g)], ringm_r.at[g])
        share(3, rows(g))

    def take_far(g):
        arrive(1, g, d3r)
        share(1, rows(g))

    spread = (10, 9, 11, 6, 14, 8, 2, 5, 7, 13, 15, 4, 12, 1, 3)
    left, right = pl.ds(0, LEFT), pl.ds(LEFT, RIGHT)

    def experts(k, count, between=()):
        span = pl.ds(k, count)
        own = blk[span].reshape(128 * count, HALF)
        gate, upper = dot_t(wexp[0], own), dot_t(wexp[2], own)
        for j in range(k, k + count):
            drain(pblk.at[j], pr.at[j])
        other = pblk[span].reshape(128 * count, HALF)
        gate, upper = gate + dot_t(wexp[1], other), upper + dot_t(wexp[3], other)
        act = (jax.nn.silu(gate) * upper).T.astype(BF16)
        for step, g in between:
            step(g)
        for cols, low, high, recv in ((right, LEFT, HALF, orh), (left, 0, LEFT, orr)):
            theirs = jnp.dot(act, wexp[5, :, low:high], preferred_element_type=F32)
            obuf[span, :, :, low:high] = theirs.reshape(count, 16, 8, high - low).astype(BF16)
            for j in range(k, k + count):
                remote(
                    obuf.at[j, :, :, cols], pout.at[j, :, :, cols], os_, recv.at[j], dev(0, 0, 0, 1 - c)
                ).start()
        ofull[span] = jnp.dot(act, wexp[4], preferred_element_type=F32).reshape(count, 16, 8, HALF)

    def send_along(k):
        drain(pout.at[k, :, :, right], orh.at[k])
        total = ofull[k, :, :, LEFT:] + pout[k, :, :, LEFT:].astype(F32)
        if k == 0:
            ghold[...] = total
            return
        rbuf[k, :, :, LEFT:] = total.astype(BF16)
        for h in (2, 3, 1, 0):
            part = pl.ds(4 * h, 4)
            remote(
                rbuf.at[k, part, :, right], gbuf.at[k - 2, part], gs, gr.at[h], dev(0, 0, XOFF[k], c)
            ).start()

    def give_back(k):
        if k == 1:
            drain(pout.at[k, :, :, right], orh.at[k])
        drain(pout.at[k, :, :, left], orr.at[k])
        high = HALF if k == 1 else LEFT
        cols = pl.ds(0, high)
        total = (ofull[k, :, :, :high] + pout[k, :, :, :high].astype(F32)).astype(BF16)
        rbuf[k, :, :, :high] = total
        ybuf[k, 0, :, :high] = total[0]
        for d in spread:
            remote(
                rbuf.at[k, d, :, cols], ybuf.at[k, d, :, cols], ys if k == 1 else yls, yr.at[k],
                dev(4 - d // 4, 4 - d % 4, 0, c),
            ).start()

    def merge(h):
        part = pl.ds(4 * h, 4)
        drain(gbuf.at[:, part], gr.at[h])
        total = ghold[part] + gbuf[0, part].astype(F32) + gbuf[1, part].astype(F32)
        gmsg[part] = total.astype(BF16)
        if h == 0:
            ybuf[0, 0, :, LEFT:] = total[0].astype(BF16)
        for d in spread:
            if d // 4 == h:
                remote(
                    gmsg.at[d], ybuf.at[0, d, :, right], ygs, ygr, dev(4 - d // 4, 4 - d % 4, 0, c)
                ).start()

    take_far(0)
    experts(0, 1, ((take_far, 1),))
    take(0)
    take_far(3)
    take_far(2)
    take(1)
    give_back(0)
    send_along(0)
    experts(1, 1)
    take(3)
    take(2)
    give_back(1)
    experts(2, 2)
    send_along(2)
    send_along(3)
    give_back(2)
    give_back(3)
    merge(3)
    merge(2)
    merge(1)
    merge(0)

    drain(table.at[pl.ds(4, 4)], trecv.at[1])
    def combine(k, low, high):
        scale = table[2 * k : 2 * k + 2].reshape(16, 128).astype(BF16)
        sums = jnp.dot(scale, ybuf[k, :, :, low:high].reshape(128, high - low), preferred_element_type=F32)
        return sums.reshape(2, SEQ, high - low).astype(BF16)

    def deliver(k, o, send, recv, cols):
        core = (c + o) % 2
        remote(
            fsend.at[2 * k + core, :, cols], fbuf.at[k, c, :, cols], send, recv, dev(0, 0, XOFF[k], core)
        ).start()

    for k in (0, 1, 2, 3):
        if k == 1:
            drain(ybuf.at[1, pl.ds(1, 15)], yr.at[1])
            fsend[2:4] = combine(1, 0, HALF)
            deliver(1, 0, fs, fr, pl.ds(0, HALF))
            deliver(1, 1, fs, fr, pl.ds(0, HALF))
            continue
        drain(ybuf.at[k, pl.ds(1, 15), :, left], yr.at[k])
        fsend[2 * k : 2 * k + 2, :, :LEFT] = combine(k, 0, LEFT)
        for o in range(2):
            if k + o > 0:
                deliver(k, o, fls, flr, left)
    drain(ybuf.at[0, pl.ds(1, 15), :, right], ygr)
    fsend[0:2, :, LEFT:] = combine(0, LEFT, HALF)
    deliver(0, 1, fgs, fgr, right)
    fbuf[0, c] = fsend[c]
    drain(fsend.at[pl.ds(0, 5), :, left], flr)
    drain(fsend.at[pl.ds(0, 2)], fr)
    drain(fsend.at[0, :, right], fgr)
    low = fbuf[0, :, :, :LEFT].astype(F32) + fbuf[3, :, :, :LEFT].astype(F32)
    low = low + fbuf[1, :, :, :LEFT].astype(F32) + fbuf[2, :, :, :LEFT].astype(F32)
    high = fbuf[0, :, :, LEFT:].astype(F32) + fbuf[1, :, :, LEFT:].astype(F32)
    total = jnp.concatenate([low, high], axis=-1)
    mixed_ref[:, :HALF] = (after[:, :HALF] + total[0]).astype(BF16)
    mixed_ref[:, HALF:] = (after[:, HALF:] + total[1]).astype(BF16)

    drain(fsend.at[pl.ds(0, 5), :, left], fls)
    drain(fsend.at[pl.ds(0, 2)], fs)
    drain(fsend.at[0, :, right], fgs)
    drain(rbuf.at[pl.ds(2, 2), :, :, right], gs)
    drain(rbuf.at[pl.ds(0, 3), pl.ds(1, 15), :, left], yls)
    drain(gmsg.at[pl.ds(1, 15)], ygs)
    drain(table.at[pl.ds(0, 7)], tsend)
    swap.wait_send()
    for copy in far:
        copy.wait_send()
    drain(msg.at[pl.ds(1, 15)], d1s)
    drain(blk.at[pl.ds(0, 2)], ring_s)
    drain(msgfar.at[pl.ds(1, 15)], d3s)
    drain(blk, ps)
    drain(obuf, os_)
    drain(rbuf.at[1, pl.ds(1, 15)], ys)


def finish(mixed_in, newk_in, newv_in, mixed_ref, newk_ref, newv_ref):
    mixed_ref[...] = mixed_in[...]
    newk_ref[...] = newk_in[...]
    newv_ref[...] = newv_in[...]


def local(*args):
    args = list(args)
    args[11], args[12] = args[11].T, args[12].T
    args[13], args[14] = jnp.swapaxes(args[13], 1, 2), jnp.swapaxes(args[14], 1, 2)
    vmem = pl.BlockSpec(memory_space=pltpu.VMEM)
    hbm = pl.BlockSpec(memory_space=pl.ANY)
    dma = pltpu.SemaphoreType.DMA
    scratch = [
        pltpu.SMEM((SEQ,), jnp.int32),
        pltpu.SMEM((HEADS,), F32),
        pltpu.VMEM((SEQ, D), BF16),
        pltpu.VMEM((D,), BF16),
        pltpu.VMEM((D,), BF16),
        pltpu.VMEM((2, SEQ), jnp.int32),
        pltpu.VMEM((2, SEQ), BF16),
        pltpu.VMEM((D, HEADS * HD), BF16),
        pltpu.VMEM((2, D, 128), BF16),
        pltpu.VMEM((SEQ, CACHE, 128), BF16),
        pltpu.VMEM((SEQ, CACHE, 128), BF16),
        pltpu.VMEM((HEADS * HD, D), BF16),
        pltpu.VMEM((6, FFD, HALF), BF16),
        pltpu.VMEM((128, 128), F32),
        pltpu.VMEM((SEQ, HEADS, CACHE), F32),
        pltpu.VMEM((SEQ, 4, HEADS, 512), BF16),
        pltpu.VMEM((512, 384), F32),
        pltpu.VMEM((128, 128), F32),
        pltpu.VMEM((8, SEQ, 128), F32),
        pltpu.VMEM((2, SEQ, HALF), BF16),
        pltpu.VMEM((SEQ, HALF), BF16),
        pltpu.VMEM((2, SEQ, HALF), BF16),
        pltpu.VMEM((16, 8, HALF), BF16),
        pltpu.VMEM((16, 8, HALF), BF16),
        pltpu.VMEM((4, 16, 8, HALF), BF16),
        pltpu.VMEM((4, 16, 8, HALF), BF16),
        pltpu.VMEM((4, 16, 8, HALF), F32),
        pltpu.VMEM((4, 16, 8, HALF), BF16),
        pltpu.VMEM((4, 16, 8, HALF), BF16),
        pltpu.VMEM((4, 16, 8, HALF), BF16),
        pltpu.VMEM((16, 8, RIGHT), F32),
        pltpu.VMEM((2, 16, 8, RIGHT), BF16),
        pltpu.VMEM((16, 8, RIGHT), BF16),
        pltpu.VMEM((4, 16, 8, HALF), BF16),
        pltpu.VMEM((8, SEQ, HALF), BF16),
        pltpu.VMEM((4, 2, SEQ, HALF), BF16),
        dma((QCHUNK + OCHUNK + 9,)), dma, dma,
        dma, dma((3,)),
        dma, dma,
        dma((2,)), dma((2,)),
        dma, dma((4,)),
        dma, dma((4,)),
        dma, dma((4,)), dma((4,)),
        dma, dma((4,)),
        dma, dma((4,)), dma((4,)),
        dma, dma, dma((4,)),
        dma, dma((4,)),
        dma, dma,
        dma, dma, dma, dma, dma, dma,
    ]
    out_shape = (
        jax.ShapeDtypeStruct((SEQ, D), BF16),
        jax.ShapeDtypeStruct((SEQ, 128), BF16),
        jax.ShapeDtypeStruct((SEQ, 128), BF16),
    )
    outs = pl.pallas_call(
        kernel,
        out_shape=tuple(pltpu.VMEM(o.shape, o.dtype) for o in out_shape),
        in_specs=[hbm] * 16,
        out_specs=(vmem, vmem, vmem),
        scratch_shapes=scratch,
        compiler_params=pltpu.CompilerParams(
            collective_id=0, has_side_effects=True, vmem_limit_bytes=60 * 2**20
        ),
        name="layer",
    )(*args)
    return pl.pallas_call(
        finish, out_shape=out_shape, in_specs=[vmem] * 3, out_specs=(vmem,) * 3, name="finish"
    )(*[pltpu.with_memory_space_constraint(o, pltpu.VMEM) for o in outs])


def solution(mesh):
    ep2, ep3 = P("ep", None), P("ep", None, None)
    in_specs = (ep2, P("ep"), ep3, ep3, P(), P(), P(), P(), P(), P(), P(), ep2, ep2, ep3, ep3, ep3)
    return jax.shard_map(
        local, mesh=mesh, in_specs=in_specs, out_specs=(ep2, ep2, ep2), check_vma=False
    )
```
